32 devices in a mesh: grp: 1, ep: 16 (over z, y, x), tp: 2 (over core).
Axes of the slice: x: 2, y: 2, z: 4, core: 2. Of those that a mesh axis runs over, the one named last changes fastest.
Arguments:
- tokens: bfloat16 [512, 2048], P(('grp', 'ep')), may hold values from -6 to 6
- in_gain: bfloat16 [2048], replicated, may hold values from 0.099609375 to 1.8984375
- route_expert: int32 [512, 6], P(('grp', 'ep')), may hold values from 0 to 15, all different within a row; in each aligned block of 32 rows (0 to 31, 32 to 63, ...) at most 16 rows name the same one
- route_weight: float32 [512, 6], P(('grp', 'ep')), may hold values from 0.05 to 1
- gate_weight: bfloat16 [16, 2048, 768], P('ep', None, 'tp'), may hold values from -0.125 to 0.125
- up_weight: bfloat16 [16, 2048, 768], P('ep', None, 'tp'), may hold values from -0.125 to 0.125
- down_weight: bfloat16 [16, 768, 2048], P('ep', 'tp'), may hold values from -1 to 1
- shared_gate: bfloat16 [2048, 768], P(None, 'tp'), may hold values from -0.125 to 0.125
- shared_up: bfloat16 [2048, 768], P(None, 'tp'), may hold values from -0.125 to 0.125
- shared_down: bfloat16 [768, 2048], P('tp'), may hold values from -1 to 1
- out_gain: bfloat16 [2048], P('tp'), may hold values from 0.099609375 to 1.8984375
Outputs:
- mixed: bfloat16 [512, 2048], P(('grp', 'ep'), 'tp')
The draws below stay inside these ranges and needn't reach their ends.
Inputs may be any that keep to these rules, and one draw needn't show every extreme that they name: `route_expert`: each row names 6 different experts. Among the rows of one device no expert is named more than 16 times, a bound that some block reaches.
All inputs are finite; a program needn't handle non-finite values.
Results may differ from the reference program's by a relative error of at most 0.0077.
Values may be sent and summed in bfloat16 or wider, within the bound.
A program may use at most 64 MiB of HBM per device.

```python
import math
import jax
import jax.numpy as jnp
import numpy as np
from jax import lax

D = 2048
FE = 768
FS = 768
TOPK = 6
TOK_DEV = 32
EXPERTS = 16
CAP = 16
TOKENS = 512
N_EP = 16
N_TP = 2


def down_matrix(key, fan_in, copies, columns):
    position = jnp.arange(columns, dtype=jnp.float32) / columns
    draws = jnp.clip(jax.random.normal(key, (copies, fan_in, columns), jnp.float32), -4.0, 4.0)
    factor = 0.5 * 3.0 ** position
    return draws * factor[None, None, :] * fan_in ** (-0.5)


def draw_down_weight(key, part):
    return down_matrix(jax.random.fold_in(key, 11), FE, EXPERTS, D).astype(jnp.bfloat16)


def draw_shared_down(key, part):
    return down_matrix(jax.random.fold_in(key, 23), FS, 1, D)[0].astype(jnp.bfloat16)


def block_scale(own_key, extent, cuts, low, top_value):
    loudness, own = 1.0, jax.random.fold_in(own_key, 6)
    for dim, shards_of in cuts:
        heights = jnp.exp(jax.random.uniform(jax.random.fold_in(own, dim), (shards_of,), jnp.float32, low / len(cuts), top_value / len(cuts)))
        loudness = loudness * jnp.repeat(heights, extent[dim] // shards_of).reshape([-1 if axis == dim else 1 for axis in range(len(extent))])
    return loudness


def shared_out(rng, own, number, rows, number_of, top, reach, skew):
    ranking = jax.random.permutation(rng, number_of)
    crowded, ordinary = portions_of(number_of, rows * top, reach, skew, True), portions_of(number_of, rows * top, reach, skew, False)
    places = jnp.arange(number_of)

    def named(lengths, offset_by):
        used = int((lengths > 0).sum())
        fixed = max(1, used // 4)
        moved = fixed + (places - fixed + offset_by * (used - fixed)) % max(1, number_of - fixed)
        return jnp.zeros((number_of,), jnp.int32).at[ranking[jnp.where(places < fixed, places, moved)]].set(jnp.asarray(lengths, jnp.int32))

    lengths = jnp.where(number % 4 == 0, named(crowded, number // 4), named(ordinary, number - number // 4 - 1))
    mixed = jax.random.permutation(jax.random.fold_in(own, 3), number_of)
    giver, receiver = mixed[0:number_of // 2 * 2:2], mixed[1:number_of // 2 * 2:2]
    slack = jnp.minimum(lengths[giver] - 1, reach - lengths[receiver]) // 2
    slack = jnp.where((giver == ranking[0]) | (receiver == ranking[0]) | (lengths[receiver] == 0), 0, jnp.maximum(slack, 0))
    moved = jax.random.randint(jax.random.fold_in(own, 4), (number_of // 2,), 0, 1 << 20) % (slack + 1)
    lengths = lengths.at[giver].add(-moved).at[receiver].add(moved)
    members = jnp.searchsorted(jnp.cumsum(lengths), jnp.arange(rows * top), side="right").astype(jnp.int32)
    grid = members.reshape(top, rows).T
    grid = grid[jax.random.permutation(jax.random.fold_in(own, 1), rows)]
    offset_by = jax.random.randint(jax.random.fold_in(own, 2), (rows, 1), 0, top)
    return jnp.take_along_axis(grid, (jnp.arange(top)[None, :] + offset_by) % top, axis=1)


def portions_of(amount, total, reach, lean, full):
    weights = [(1 << 20) // math.isqrt(grade ** lean) + 1 for grade in range(1, amount + 1)]
    largest = reach if full else min(reach, max(-(-total // amount), total * weights[0] // sum(weights)))
    least = 1 if total - largest >= amount - 1 else 0
    holding, rest = [largest] + [least] * (amount - 1), total - largest - least * (amount - 1)
    while rest > 0:
        free = [i for i in range(1, amount) if holding[i] < largest] or [i for i in range(1, amount) if holding[i] < reach]
        pool, left = sum([weights[i] for i in free]), rest
        for i in free:
            extra = min(reach - holding[i], max(1, left * weights[i] // pool), rest)
            holding[i] = holding[i] + extra
            rest = rest - extra
    return np.array(holding)


def scatter_about(key, shape, spread, reach, shards=(), kind=jnp.bfloat16):
    loudness = block_scale(key, shape, shards, -0.22, 0.18) if shards else 1.0
    array = jax.random.normal(key, shape, jnp.float32) * spread * loudness
    return jnp.minimum(jnp.maximum(array, -reach), reach).astype(kind)


def setup_inputs(seed: int = 0, part: int = 0) -> dict:
    keys = jax.random.split(jax.random.key(seed), 12)
    own_keys = jax.random.split(jax.random.fold_in(keys[11], part), 12)
    tokens = scatter_about(own_keys[0], (TOKENS, D), 1.0, 6.0, ((0, 16),))
    in_gain = jnp.clip(1.0 + 0.18 * jax.random.normal(keys[1], (D,), jnp.float32), 0.099609375, 1.8984375).astype(jnp.bfloat16)
    route_expert_keys = jax.random.split(jax.random.fold_in(own_keys[2], 1), TOKENS // TOK_DEV)
    route_expert_turns = jax.random.permutation(jax.random.fold_in(own_keys[2], 3), TOKENS // TOK_DEV)
    route_expert = jax.vmap(lambda own, number: shared_out(jax.random.fold_in(own_keys[2], 2), own, number, TOK_DEV, EXPERTS, TOPK, CAP, 2))(route_expert_keys, route_expert_turns).reshape((TOKENS, TOPK))
    route_weight = jnp.clip(jnp.exp(math.log(1.0) - 2.9957323 * jax.random.uniform(own_keys[3], (TOKENS, TOPK), jnp.float32) ** block_scale(own_keys[3], (TOKENS, TOPK), ((0, 16),), -0.2, 0.2)), 0.05, 1.0)
    gate_weight = scatter_about(keys[4], (EXPERTS, D, FE), D ** -0.5, 0.125, ((0, 16), (2, 2)))
    up_weight = scatter_about(keys[5], (EXPERTS, D, FE), D ** -0.5, 0.125, ((0, 16), (2, 2)))
    down_weight = draw_down_weight(jax.random.fold_in(keys[11], 71), part)
    shared_gate = scatter_about(keys[7], (D, FS), D ** -0.5, 0.125, ((1, 2),))
    shared_up = scatter_about(keys[8], (D, FS), D ** -0.5, 0.125, ((1, 2),))
    shared_down = draw_shared_down(jax.random.fold_in(keys[11], 71), part)
    out_gain = jnp.clip(1.0 + 0.18 * jax.random.normal(keys[10], (D,), jnp.float32), 0.099609375, 1.8984375).astype(jnp.bfloat16)
    return dict(tokens=tokens, in_gain=in_gain, route_expert=route_expert, route_weight=route_weight, gate_weight=gate_weight, up_weight=up_weight, down_weight=down_weight, shared_gate=shared_gate, shared_up=shared_up, shared_down=shared_down, out_gain=out_gain)


EPSILON = 1e-06

def normalize(values, gain_vector):
    floats = values.astype(jnp.float32)
    scaled = floats * lax.rsqrt(lax.optimization_barrier(jnp.mean(floats * floats, axis=-1, keepdims=True)) + EPSILON)
    return (scaled * gain_vector.astype(jnp.float32)).astype(jnp.bfloat16)

def swiglu_hidden(inputs, gate_here, up_here):
    gate_value = jnp.dot(inputs, gate_here, preferred_element_type=jnp.float32)
    upward = jnp.dot(inputs, up_here, preferred_element_type=jnp.float32)
    return (jax.nn.silu(gate_value) * upward).astype(jnp.bfloat16)

def split_product(hidden, down_here, pieces):
    inner_width = hidden.shape[1] // pieces
    running = jnp.zeros((hidden.shape[0], down_here.shape[1]), jnp.float32)
    for portion in range(pieces):
        partial_value = jnp.dot(hidden[:, portion * inner_width:(portion + 1) * inner_width], down_here[portion * inner_width:(portion + 1) * inner_width], preferred_element_type=jnp.float32)
        running = running + lax.optimization_barrier(partial_value.astype(jnp.bfloat16)).astype(jnp.float32)
    return running.astype(jnp.bfloat16)

def slot_tables(routes_here, experts, capacity):
    picked_count = routes_here.shape[0] * routes_here.shape[1]
    flattened = routes_here.reshape(picked_count).astype(jnp.int32)
    onehot = (flattened[:, None] == jnp.arange(experts, dtype=jnp.int32)[None, :]).astype(jnp.int32)
    earlier = (jnp.cumsum(onehot, axis=0) - onehot).astype(jnp.int32)
    ranked = lax.optimization_barrier(jnp.sum(earlier * onehot, axis=1)).astype(jnp.int32)
    slot_index = flattened * capacity + ranked
    source_token = jnp.arange(picked_count, dtype=jnp.int32) // routes_here.shape[1]
    matches = slot_index[None, :] == jnp.arange(experts * capacity, dtype=jnp.int32)[:, None]
    filled = jnp.any(matches, axis=1)
    slot_owner = lax.optimization_barrier(jnp.sum(jnp.where(matches, source_token[None, :], 0), axis=1)).astype(jnp.int32)
    return (slot_index, filled, slot_owner)

def reference(tokens, in_gain, route_expert, route_weight, gate_weight, up_weight, down_weight, shared_gate, shared_up, shared_down, out_gain):
    capacity = CAP
    normed = normalize(tokens, in_gain)
    grouped = route_expert.reshape(N_EP, TOK_DEV, TOPK)
    slot_index, filled, slot_owner = jax.vmap(lambda routes_here: slot_tables(routes_here, EXPERTS, capacity))(grouped)
    per_device = normed.reshape(N_EP, TOK_DEV, D)
    outgoing = jax.vmap(lambda rows_here, chosen, filled_here: jnp.where(filled_here[:, None], rows_here[chosen], jnp.zeros((), jnp.bfloat16)))(per_device, slot_owner, filled)
    by_expert = outgoing.reshape(N_EP, EXPERTS, capacity, D).transpose(1, 0, 2, 3).reshape(EXPERTS, N_EP * capacity, D)

    def expert_pass(inputs):
        expert_rows, gate_here, up_here, down_here = inputs
        return split_product(swiglu_hidden(expert_rows, gate_here, up_here), down_here, N_TP)
    results = lax.map(expert_pass, (by_expert, gate_weight, up_weight, down_weight))
    returned = results.reshape(EXPERTS, N_EP, capacity, D).transpose(1, 0, 2, 3).reshape(N_EP, EXPERTS * capacity, D)
    picked = jax.vmap(lambda result_rows, chosen: result_rows[chosen])(returned, slot_index).astype(jnp.float32)
    picked = picked * route_weight.reshape(N_EP, TOK_DEV * TOPK)[:, :, None]
    routed = lax.optimization_barrier(jnp.sum(picked.reshape(TOKENS, TOPK, D), axis=1))
    shared = split_product(swiglu_hidden(normed, shared_gate, shared_up), shared_down, N_TP).astype(jnp.float32)
    combined = shared + routed
    scaled = combined * lax.rsqrt(lax.optimization_barrier(jnp.mean(combined * combined, axis=1, keepdims=True)) + EPSILON)
    return (scaled * out_gain.astype(jnp.float32)).astype(jnp.bfloat16)
```

```python
import functools

import jax
import jax.numpy as jnp
from jax import lax
from jax.experimental import pallas as pl
from jax.experimental.pallas import tpu as pltpu
from jax.sharding import PartitionSpec as P

EPSILON = 1e-06
F32 = jnp.float32
BF16 = jnp.bfloat16


def dot(a, b):
    return jnp.dot(a, b, preferred_element_type=F32)


def dot_t(a, b):
    return lax.dot_general(a, b, (((1,), (1,)), ((), ())), preferred_element_type=F32)


def silu_product(gate_value, upward):
    return (gate_value * (1.0 / (1.0 + jnp.exp(-gate_value))) * upward).astype(BF16)


def kernel(
    outer,
    inner,
    cap,
    info_width,
    split,
    relay,
    tokens_hbm,
    in_gain_hbm,
    route_expert_hbm,
    route_weight_hbm,
    out_gain_hbm,
    gate_hbm,
    up_hbm,
    down_hbm,
    sgate_hbm,
    sup_hbm,
    sdown_hbm,
    mixed,
    tokens,
    in_gain,
    route_expert,
    route_weight,
    out_gain,
    gate_w,
    up_w,
    down_w,
    sgate_w,
    sup_w,
    sdown_w,
    normed,
    column,
    staged,
    rows_in,
    part_out,
    part_in,
    part_own,
    result,
    back,
    sum_out,
    sum_in,
    shared_out,
    shared_in,
    last_out,
    last_in,
    w_sem,
    col_send,
    col_recv,
    col_pass,
    plane_recv,
    pair_recv,
    part_recv,
    back_recv,
    sum_recv,
    send_sem,
    core_sem,
):
    ep = lax.axis_index("ep")
    tp = lax.axis_index("tp")
    z = ep // inner
    p = ep % inner
    experts = outer * inner
    local_tokens, width = tokens.shape
    half = width // 2

    loads = [
        pltpu.make_async_copy(src, dst, w_sem.at[i])
        for i, (src, dst) in enumerate(
            [
                (tokens_hbm, tokens),
                (in_gain_hbm, in_gain),
                (route_expert_hbm, route_expert),
                (route_weight_hbm, route_weight),
                (out_gain_hbm, out_gain),
                (sgate_hbm, sgate_w),
                (sup_hbm, sup_w),
                (sdown_hbm, sdown_w),
                (gate_hbm.at[0], gate_w),
                (up_hbm.at[0], up_w),
                (down_hbm.at[0], down_w),
            ]
        )
    ]
    for load in loads[:5]:
        load.start()

    barrier = pltpu.get_barrier_semaphore()

    def greet(ep_to, tp_to):
        pl.semaphore_signal(
            barrier, inc=1, device_id={"ep": ep_to, "tp": tp_to}, device_id_type=pl.DeviceIdType.MESH
        )

    for d in range(1, outer):
        greet(lax.rem(z + d, outer) * inner + p, tp)
    for d in range(1, inner):
        greet(z * inner + lax.rem(p + d, inner), tp)
    greet(ep, 1 - tp)

    for load in loads[:5]:
        load.wait()
    for load in loads[5:]:
        load.start()
    floats = tokens[...].astype(F32)
    mean = jnp.sum(floats * floats, axis=1, keepdims=True) / width
    rows = (floats * lax.rsqrt(mean + EPSILON) * in_gain[...].astype(F32)[None, :]).astype(BF16)
    normed[...] = rows

    fact = lax.broadcasted_iota(jnp.int32, (info_width, local_tokens), 0)
    fact_expert = lax.rem(fact, experts)
    named = jnp.zeros((info_width, local_tokens), F32)
    weight = jnp.zeros((info_width, local_tokens), F32)
    for k in range(route_expert.shape[0]):
        hit = route_expert[k : k + 1, :] == fact_expert
        named = named + jnp.where(hit, 1.0, 0.0)
        weight = weight + jnp.where(hit, route_weight[k : k + 1, :], 0.0)
    row_i = lax.broadcasted_iota(jnp.int32, (local_tokens, local_tokens), 0)
    col_i = lax.broadcasted_iota(jnp.int32, (local_tokens, local_tokens), 1)
    upto = jnp.where(row_i <= col_i, 1.0, 0.0).astype(BF16)
    place = dot(named.astype(BF16), upto) * named
    high = weight.astype(BF16).astype(F32)
    facts = jnp.where(fact < experts, place, jnp.where(fact < 2 * experts, high, weight - high))
    facts = jnp.where(fact < 3 * experts, facts, 0.0).astype(BF16)
    same = jnp.where(row_i == col_i, 1.0, 0.0).astype(BF16)
    info = dot_t(same, facts).astype(BF16)

    short = jnp.minimum(z, outer - 1 - z)

    def nth(i):
        if i == 0:
            return z
        near = (i + 1) // 2 if i % 2 else -(i // 2)
        far = jnp.where(z < outer - 1 - z, i - short, short - i)
        return z + jnp.where(i <= 2 * short, near, far)

    order = [nth(i) for i in range(outer)]

    def direct(to):
        if not relay:
            return z >= 0
        return (to - z) * (to - z) != 4

    def passes(j):
        on = 2 * z - j
        return on, ((j - z) * (j - z) == 1) & (on >= 0) & (on < outer)

    slots = inner * cap
    slot_row = lax.broadcasted_iota(jnp.int32, (slots, info_width), 0)
    slot_lane = lax.broadcasted_iota(jnp.int32, (slots, info_width), 1)
    slot_expert = z * inner + slot_row // cap

    def selector(offset):
        return jnp.where(slot_lane == slot_expert + offset, 1.0, 0.0).astype(BF16)

    slot_rank = (lax.broadcasted_iota(jnp.int32, (slots, local_tokens), 0) % cap + 1).astype(F32)
    slot_of_lane = (lax.broadcasted_iota(jnp.int32, (local_tokens, slots), 1) % cap + 1).astype(F32)
    peers = [lax.rem(p + e, inner) for e in range(1, inner)]

    pl.semaphore_wait(barrier, outer + inner - 1)

    def on_core(core):
        edges = (0, split, width)
        first, end = edges[core], edges[core + 1]
        count = end - first
        other = 1 - core
        mine = pl.ds(first, count)
        theirs = pl.ds(edges[other], edges[other + 1] - edges[other])
        facts_at = pl.ds(first, info_width)
        rows_at = pl.ds(first + info_width, count)
        sent_at = pl.ds(first, info_width + count)

        def pieces(which):
            begin, stop = edges[which], edges[which + 1]
            parts = PIECES[which] if (stop - begin) % (128 * PIECES[which]) == 0 else 1
            size = (stop - begin) // parts
            return [pl.ds(begin + n * size, size) for n in range(parts)]

        my_pieces = pieces(core)

        column[z, :, facts_at] = info
        column[z, :, rows_at] = rows[:, first:end]

        def remote(src, dst, send, recv, ep_to, tp_to):
            return pltpu.make_async_remote_copy(
                src_ref=src,
                dst_ref=dst,
                send_sem=send,
                recv_sem=recv,
                device_id={"ep": ep_to, "tp": tp_to},
                device_id_type=pl.DeviceIdType.MESH,
            )

        def send(src, dst, kind, recv_sem, ep_to, tp_to):
            remote(src, dst, send_sem.at[kind], recv_sem, ep_to, tp_to).start()

        def arrive(ref, recv_sem):
            with jax.named_scope("w"):
                remote(ref, ref, send_sem.at[0], recv_sem, ep, other).wait_recv()

        def sent(ref, kind):
            remote(ref, ref, send_sem.at[kind], col_recv.at[0], ep, other).wait_send()

        def column_copy(block, to, sem):
            here = column.at[block, :, sent_at]
            return remote(here, here, sem, col_recv.at[block], to * inner + p, core)

        for to in order[1:]:

            @pl.when(direct(to))
            def _(to=to):
                column_copy(z, to, col_send.at[to]).start()

        pick_place = selector(0)
        pick_high = selector(experts)
        pick_low = selector(2 * experts)

        def dispatch(i):
            j = order[i]
            if i:
                arrive(column.at[j, :, sent_at], col_recv.at[j])
                if relay:
                    on, wanted = passes(j)

                    @pl.when(wanted)
                    def _():
                        column_copy(j, on, col_pass.at[j]).start()

            where = dot_t(pick_place, column[j, :, facts_at])
            onehot = jnp.where(where == slot_rank, 1.0, 0.0).astype(BF16)
            moved = dot(onehot, column[j, :, rows_at]).astype(BF16)
            staged[j, :, :, mine] = moved.reshape(inner, cap, count)
            for to in peers:
                send(
                    staged.at[j, to, :, mine],
                    rows_in.at[j, p, :, mine],
                    0,
                    plane_recv.at[j],
                    z * inner + to,
                    core,
                )
            rows_in[j, p, :, mine] = staged[j, p, :, mine]

        def pair(i):
            j = order[i]
            arrive(rows_in.at[j, pl.ds(0, inner - 1), :, mine], plane_recv.at[j])
            here = rows_in.at[j, :, :, mine]
            send(here, here, 1, pair_recv.at[j], ep, other)

        def expert(*group):
            if group[0] == 0:
                for load in loads[8:]:
                    load.wait()

            def rows_of(columns):
                blocks = [rows_in[order[i], :, :, columns].reshape(slots, columns.size) for i in group]
                return blocks[0] if len(blocks) == 1 else jnp.concatenate(blocks, axis=0)

            own_rows = rows_of(mine)
            gate_value = dot(own_rows, gate_w[mine, :])
            upward = dot(own_rows, up_w[mine, :])
            for i in group:
                j = order[i]
                arrive(rows_in.at[j, :, :, theirs], pair_recv.at[j])
            other_rows = rows_of(theirs)
            gate_value = gate_value + dot(other_rows, gate_w[theirs, :])
            upward = upward + dot(other_rows, up_w[theirs, :])
            hidden = silu_product(gate_value, upward)

            def store(target, columns):
                values = dot(hidden, down_w[:, columns]).astype(BF16)
                for n, i in enumerate(group):
                    block = values[n * slots : (n + 1) * slots]
                    target[order[i], :, :, columns] = block.reshape(inner, cap, columns.size)

            for n, piece in enumerate(pieces(other)):
                store(part_out, piece)
                for i in reversed(group):
                    j = order[i]
                    here = part_out.at[j, :, :, piece]
                    send(here, part_in.at[j, :, :, piece], 2, part_recv.at[j, n], ep, other)
            for piece in my_pieces:
                store(part_own, piece)

        def give_back(i):
            j = order[i]
            for n, piece in enumerate(my_pieces):
                arrive(part_in.at[j, :, :, piece], part_recv.at[j, n])
                total = part_own[j, :, :, piece].astype(F32) + part_in[j, :, :, piece].astype(F32)
                result[j, :, :, piece] = total.astype(BF16)
                for to in peers:
                    send(
                        result.at[j, to, :, piece],
                        back.at[j, p, :, piece],
                        3,
                        back_recv.at[j, n],
                        z * inner + to,
                        core,
                    )
                back[j, p, :, piece] = result[j, p, :, piece]

        def weigh(i):
            known = column[order[i], :, facts_at]
            chosen = dot_t(known, pick_place) == slot_of_lane
            high_part = jnp.where(chosen, dot_t(known, pick_high), 0.0).astype(BF16)
            low_part = jnp.where(chosen, dot_t(known, pick_low), 0.0).astype(BF16)
            return high_part, low_part

        def gathered(i, weights, n, piece):
            j = order[i]
            arrive(back.at[j, pl.ds(0, inner - 1), :, piece], back_recv.at[j, n])
            values = back[j, :, :, piece].reshape(slots, piece.size)
            return dot(weights[0], values) + dot(weights[1], values)

        def combine(i):
            j = order[i]
            weights = weigh(i)
            for n, piece in enumerate(my_pieces):
                sum_out[i - 1, :, piece] = gathered(i, weights, n, piece).astype(BF16)
                here = sum_out.at[i - 1, :, piece]
                send(here, sum_in.at[z, :, piece], 4, sum_recv.at[z, n], j * inner + p, core)

        def shared():
            for load in loads[5:8]:
                load.wait()
            inputs = normed[...]
            hidden = silu_product(dot(inputs, sgate_w[...]), dot(inputs, sup_w[...]))
            shared_out[:, theirs] = dot(hidden, sdown_w[:, theirs]).astype(BF16)
            here = shared_out.at[:, theirs]
            send(here, shared_in.at[:, theirs], 5, core_sem.at[0], ep, other)
            shared_out[:, mine] = dot(hidden, sdown_w[:, mine]).astype(BF16)

        def step(task, *what):
            with jax.named_scope(task.__name__ + "".join(str(w) for w in what)):
                task(*what)

        for task, *what in PLAN(outer, dispatch, shared, pair, expert, give_back, combine):
            step(task, *what)

        totals = []
        with jax.named_scope("own"):
            weights = weigh(0)
            arrive(shared_in.at[:, mine], core_sem.at[0])
            for n, piece in enumerate(my_pieces):
                shared_rows = shared_out[:, piece].astype(F32) + shared_in[:, piece].astype(F32)
                totals.append(gathered(0, weights, n, piece) + shared_rows.astype(BF16).astype(F32))
        with jax.named_scope("sums"):
            for i in range(1, outer):
                j = order[i]
                for n, piece in enumerate(my_pieces):
                    arrive(sum_in.at[j, :, piece], sum_recv.at[j, n])
                    totals[n] = totals[n] + sum_in[j, :, piece].astype(F32)
        combined = totals[0] if len(totals) == 1 else jnp.concatenate(totals, axis=1)

        lanes = last_out.shape[1] - (half - split)
        squares_at = pl.ds(half - split, lanes)
        own_squares = jnp.sum(combined * combined, axis=1, keepdims=True)
        last_out[:, squares_at] = jnp.broadcast_to(own_squares, (local_tokens, lanes))
        if core == 0:
            leaving, coming = squares_at, pl.ds(0, half - split + lanes)
        else:
            leaving, coming = pl.ds(0, half - split + lanes), squares_at
            if half > split:
                last_out[:, : half - split] = combined[:, : half - split]
        here = last_out.at[:, leaving]
        send(here, last_in.at[:, leaving], 6, core_sem.at[1], ep, other)
        with jax.named_scope("lastwait"):
            arrive(last_in.at[:, coming], core_sem.at[1])
        squares = own_squares + last_in[:, half - split : half - split + 1]
        scale = lax.rsqrt(squares / width + EPSILON)
        gain = out_gain[...].astype(F32)[None, :]
        if core == 0:
            mixed[:, :split] = (combined * scale * gain[:, :split]).astype(BF16)
            if half > split:
                extra = last_in[:, : half - split] * scale * gain[:, split:]
                mixed[:, split:] = extra.astype(BF16)
        else:
            mixed[...] = (combined[:, half - split :] * scale * gain).astype(BF16)

        for to in order[1:]:

            @pl.when(direct(to))
            def _(to=to):
                column_copy(z, to, col_send.at[to]).wait_send()

            if relay:
                on, wanted = passes(to)

                @pl.when(wanted)
                def _(to=to, on=on):
                    column_copy(to, on, col_pass.at[to]).wait_send()

        sent(staged.at[:, pl.ds(0, inner - 1), :, mine], 0)
        sent(rows_in.at[:, :, :, mine], 1)
        sent(part_out.at[:, :, :, theirs], 2)
        sent(result.at[:, pl.ds(0, inner - 1), :, mine], 3)
        sent(sum_out.at[:, :, mine], 4)
        sent(shared_out.at[:, theirs], 5)
        sent(here, 6)

    for core in range(2):

        @pl.when(tp == core)
        def _(core=core):
            on_core(core)


def plan(outer, dispatch, shared, pair, expert, give_back, combine):
    steps = [(dispatch, 0), (shared,), (dispatch, 1)]
    for i in range(2, outer):
        steps += [(dispatch, i), (pair, i - 2)]
    steps += [(pair, outer - 2), (expert, 0, 1)]
    for i in range(2, outer):
        steps += [(give_back, 1), (give_back, 0)] if i == 2 else [(give_back, i - 1)]
        steps += [(pair, outer - 1)] if i == outer - 1 else []
        steps += [(expert, i)]
    steps += [(give_back, outer - 1)]
    steps += [(combine, i) for i in range(1, outer)]
    return steps


PLAN = plan
PIECES = (1, 2)
SPLIT = 4
RELAY = True


def body(
    experts,
    tokens,
    in_gain,
    route_expert,
    route_weight,
    gate_weight,
    up_weight,
    down_weight,
    shared_gate,
    shared_up,
    shared_down,
    out_gain,
):
    inner = 1
    while inner * inner < experts:
        inner *= 2
    outer = experts // inner
    local_tokens, width = tokens.shape
    half = width // 2
    split = width * SPLIT // 16
    top_count = route_expert.shape[1]
    capacity = max(2, (local_tokens * top_count * 4 + 3 * experts - 1) // (3 * experts))
    cap = -(-capacity // 16) * 16
    info_width = -(-3 * experts // 128) * 128
    hidden = gate_weight.shape[2]
    shared_width = shared_gate.shape[1]

    def vm(shape, kind=BF16):
        return pltpu.VMEM(shape, kind)

    grid_rows = (outer, inner, cap, width)
    most = max(PIECES)
    dma = pltpu.SemaphoreType.DMA
    in_vmem = pl.BlockSpec(memory_space=pltpu.VMEM)
    in_hbm = pl.BlockSpec(memory_space=pltpu.HBM)
    return pl.pallas_call(
        functools.partial(kernel, outer, inner, cap, info_width, split, RELAY),
        out_shape=pltpu.VMEM((local_tokens, half), BF16),
        in_specs=[in_hbm] * 11,
        out_specs=in_vmem,
        scratch_shapes=[
            vm((local_tokens, width)),
            vm((width,)),
            vm((top_count, local_tokens), jnp.int32),
            vm((top_count, local_tokens), F32),
            vm((half,)),
            vm((width, hidden)),
            vm((width, hidden)),
            vm((hidden, width)),
            vm((width, shared_width)),
            vm((width, shared_width)),
            vm((shared_width, width)),
            vm((local_tokens, width)),
            vm((outer, local_tokens, width + info_width)),
            vm(grid_rows),
            vm(grid_rows),
            vm(grid_rows),
            vm(grid_rows),
            vm(grid_rows),
            vm(grid_rows),
            vm(grid_rows),
            vm((outer - 1, local_tokens, width)),
            vm((outer, local_tokens, width)),
            vm((local_tokens, width)),
            vm((local_tokens, width)),
            vm((local_tokens, half - split + 128), F32),
            vm((local_tokens, half - split + 128), F32),
            dma((11,)),
            dma((outer,)),
            dma((outer,)),
            dma((outer,)),
            dma((outer,)),
            dma((outer,)),
            dma((outer, most)),
            dma((outer, most)),
            dma((outer, most)),
            dma((7,)),
            dma((2,)),
        ],
        compiler_params=pltpu.CompilerParams(
            collective_id=0, has_side_effects=True, vmem_limit_bytes=60 * 1024 * 1024
        ),
    )(
        tokens,
        in_gain,
        route_expert.T,
        route_weight.T,
        out_gain,
        gate_weight,
        up_weight,
        down_weight,
        shared_gate,
        shared_up,
        shared_down,
    )


def solution(mesh):
    return jax.shard_map(
        functools.partial(body, mesh.shape["ep"]),
        mesh=mesh,
        in_specs=(
            P(("grp", "ep"), None),
            P(),
            P(("grp", "ep"), None),
            P(("grp", "ep"), None),
            P("ep", None, "tp"),
            P("ep", None, "tp"),
            P("ep", "tp", None),
            P(None, "tp"),
            P(None, "tp"),
            P("tp", None),
            P("tp"),
        ),
        out_specs=P(("grp", "ep"), "tp"),
        check_vma=False,
    )
```

```python
import functools

import jax
import jax.numpy as jnp
from jax import lax
from jax.experimental import pallas as pl
from jax.experimental.pallas import tpu as pltpu
from jax.sharding import PartitionSpec as P

EPSILON = 1e-06
F32 = jnp.float32
BF16 = jnp.bfloat16


def dot(a, b):
    return jnp.dot(a, b, preferred_element_type=F32)


def dot_t(a, b):
    return lax.dot_general(a, b, (((1,), (1,)), ((), ())), preferred_element_type=F32)


def silu_product(gate_value, upward):
    return (gate_value * (1.0 / (1.0 + jnp.exp(-gate_value))) * upward).astype(BF16)


def kernel(
    outer,
    inner,
    cap,
    info_width,
    split,
    relay,
    tokens_hbm,
    in_gain_hbm,
    route_expert_hbm,
    route_weight_hbm,
    out_gain_hbm,
    gate_hbm,
    up_hbm,
    down_hbm,
    sgate_hbm,
    sup_hbm,
    sdown_hbm,
    mixed,
    tokens,
    in_gain,
    route_expert,
    route_weight,
    out_gain,
    gate_w,
    up_w,
    down_w,
    sgate_w,
    sup_w,
    sdown_w,
    normed,
    column,
    staged,
    rows_in,
    part_out,
    part_in,
    part_own,
    result,
    back,
    sum_out,
    sum_in,
    shared_out,
    shared_in,
    last_out,
    last_in,
    w_sem,
    col_send,
    col_recv,
    col_pass,
    plane_recv,
    pair_recv,
    part_recv,
    back_recv,
    sum_recv,
    send_sem,
    core_sem,
):
    ep = lax.axis_index("ep")
    tp = lax.axis_index("tp")
    z = ep // inner
    p = ep % inner
    experts = outer * inner
    local_tokens, width = tokens.shape
    half = width // 2

    loads = [
        pltpu.make_async_copy(src, dst, w_sem.at[i])
        for i, (src, dst) in enumerate(
            [
                (tokens_hbm, tokens),
                (in_gain_hbm, in_gain),
                (route_expert_hbm, route_expert),
                (route_weight_hbm, route_weight),
                (out_gain_hbm, out_gain),
                (sgate_hbm, sgate_w),
                (sup_hbm, sup_w),
                (sdown_hbm, sdown_w),
                (gate_hbm.at[0], gate_w),
                (up_hbm.at[0], up_w),
                (down_hbm.at[0], down_w),
            ]
        )
    ]
    for load in loads[:5]:
        load.start()

    barrier = pltpu.get_barrier_semaphore()

    def greet(ep_to, tp_to):
        pl.semaphore_signal(
            barrier, inc=1, device_id={"ep": ep_to, "tp": tp_to}, device_id_type=pl.DeviceIdType.MESH
        )

    for d in range(1, outer):
        greet(lax.rem(z + d, outer) * inner + p, tp)
    for d in range(1, inner):
        greet(z * inner + lax.rem(p + d, inner), tp)
    greet(ep, 1 - tp)

    for load in loads[:5]:
        load.wait()
    for load in loads[5:]:
        load.start()
    floats = tokens[...].astype(F32)
    mean = jnp.sum(floats * floats, axis=1, keepdims=True) / width
    rows = (floats * lax.rsqrt(mean + EPSILON) * in_gain[...].astype(F32)[None, :]).astype(BF16)
    normed[...] = rows

    fact = lax.broadcasted_iota(jnp.int32, (info_width, local_tokens), 0)
    fact_expert = lax.rem(fact, experts)
    named = jnp.zeros((info_width, local_tokens), F32)
    weight = jnp.zeros((info_width, local_tokens), F32)
    for k in range(route_expert.shape[0]):
        hit = route_expert[k : k + 1, :] == fact_expert
        named = named + jnp.where(hit, 1.0, 0.0)
        weight = weight + jnp.where(hit, route_weight[k : k + 1, :], 0.0)
    row_i = lax.broadcasted_iota(jnp.int32, (local_tokens, local_tokens), 0)
    col_i = lax.broadcasted_iota(jnp.int32, (local_tokens, local_tokens), 1)
    upto = jnp.where(row_i <= col_i, 1.0, 0.0).astype(BF16)
    place = dot(named.astype(BF16), upto) * named
    high = weight.astype(BF16).astype(F32)
    facts = jnp.where(fact < experts, place, jnp.where(fact < 2 * experts, high, weight - high))
    facts = jnp.where(fact < 3 * experts, facts, 0.0).astype(BF16)
    same = jnp.where(row_i == col_i, 1.0, 0.0).astype(BF16)
    info = dot_t(same, facts).astype(BF16)

    short = jnp.minimum(z, outer - 1 - z)

    def nth(i):
        if i == 0:
            return z
        near = (i + 1) // 2 if i % 2 else -(i // 2)
        far = jnp.where(z < outer - 1 - z, i - short, short - i)
        if i > 1:
            ends = i + 1 if i < outer - 1 else 2
            far = jnp.where(short > 0, far, jnp.where(z == 0, ends, -ends))
        return z + jnp.where(i <= 2 * short, near, far)

    order = [nth(i) for i in range(outer)]

    def direct(to):
        if not relay:
            return z >= 0
        return (to - z) * (to - z) != 4

    def passes(j):
        on = 2 * z - j
        return on, ((j - z) * (j - z) == 1) & (on >= 0) & (on < outer)

    slots = inner * cap
    slot_row = lax.broadcasted_iota(jnp.int32, (slots, info_width), 0)
    slot_lane = lax.broadcasted_iota(jnp.int32, (slots, info_width), 1)
    slot_expert = z * inner + slot_row // cap

    def selector(offset):
        return jnp.where(slot_lane == slot_expert + offset, 1.0, 0.0).astype(BF16)

    slot_rank = (lax.broadcasted_iota(jnp.int32, (slots, local_tokens), 0) % cap + 1).astype(F32)
    slot_of_lane = (lax.broadcasted_iota(jnp.int32, (local_tokens, slots), 1) % cap + 1).astype(F32)
    peers = [lax.rem(p + e, inner) for e in range(1, inner)]

    pl.semaphore_wait(barrier, outer + inner - 1)

    def on_core(core):
        edges = (0, split, width)
        first, end = edges[core], edges[core + 1]
        count = end - first
        other = 1 - core
        mine = pl.ds(first, count)
        theirs = pl.ds(edges[other], edges[other + 1] - edges[other])
        facts_at = pl.ds(first, info_width)
        rows_at = pl.ds(first + info_width, count)
        sent_at = pl.ds(first, info_width + count)

        def pieces(which):
            begin, stop = edges[which], edges[which + 1]
            parts = PIECES[which] if (stop - begin) % (128 * PIECES[which]) == 0 else 1
            size = (stop - begin) // parts
            return [pl.ds(begin + n * size, size) for n in range(parts)]

        my_pieces = pieces(core)

        column[z, :, facts_at] = info
        column[z, :, rows_at] = rows[:, first:end]

        def remote(src, dst, send, recv, ep_to, tp_to):
            return pltpu.make_async_remote_copy(
                src_ref=src,
                dst_ref=dst,
                send_sem=send,
                recv_sem=recv,
                device_id={"ep": ep_to, "tp": tp_to},
                device_id_type=pl.DeviceIdType.MESH,
            )

        def send(src, dst, kind, recv_sem, ep_to, tp_to):
            remote(src, dst, send_sem.at[kind], recv_sem, ep_to, tp_to).start()

        def arrive(ref, recv_sem):
            with jax.named_scope("w"):
                remote(ref, ref, send_sem.at[0], recv_sem, ep, other).wait_recv()

        def sent(ref, kind):
            remote(ref, ref, send_sem.at[kind], col_recv.at[0], ep, other).wait_send()

        def column_copy(block, to, sem):
            here = column.at[block, :, sent_at]
            return remote(here, here, sem, col_recv.at[block], to * inner + p, core)

        for to in order[1:]:

            @pl.when(direct(to))
            def _(to=to):
                column_copy(z, to, col_send.at[to]).start()

        pick_place = selector(0)
        pick_high = selector(experts)
        pick_low = selector(2 * experts)

        def dispatch(i):
            j = order[i]
            if i:
                arrive(column.at[j, :, sent_at], col_recv.at[j])
                if relay:
                    on, wanted = passes(j)

                    @pl.when(wanted)
                    def _():
                        column_copy(j, on, col_pass.at[j]).start()

            where = dot_t(pick_place, column[j, :, facts_at])
            onehot = jnp.where(where == slot_rank, 1.0, 0.0).astype(BF16)
            moved = dot(onehot, column[j, :, rows_at]).astype(BF16)
            staged[j, :, :, mine] = moved.reshape(inner, cap, count)
            for to in peers:
                send(
                    staged.at[j, to, :, mine],
                    rows_in.at[j, p, :, mine],
                    0,
                    plane_recv.at[j],
                    z * inner + to,
                    core,
                )
            rows_in[j, p, :, mine] = staged[j, p, :, mine]

        def pair(i):
            j = order[i]
            arrive(rows_in.at[j, pl.ds(0, inner - 1), :, mine], plane_recv.at[j])
            here = rows_in.at[j, :, :, mine]
            send(here, here, 1, pair_recv.at[j], ep, other)

        def expert(*group):
            if group[0] == 0:
                for load in loads[8:]:
                    load.wait()

            def rows_of(columns):
                blocks = [rows_in[order[i], :, :, columns].reshape(slots, columns.size) for i in group]
                return blocks[0] if len(blocks) == 1 else jnp.concatenate(blocks, axis=0)

            own_rows = rows_of(mine)
            gate_value = dot(own_rows, gate_w[mine, :])
            upward = dot(own_rows, up_w[mine, :])
            for i in group:
                j = order[i]
                arrive(rows_in.at[j, :, :, theirs], pair_recv.at[j])
            other_rows = rows_of(theirs)
            gate_value = gate_value + dot(other_rows, gate_w[theirs, :])
            upward = upward + dot(other_rows, up_w[theirs, :])
            hidden = silu_product(gate_value, upward)

            def store(target, columns):
                values = dot(hidden, down_w[:, columns]).astype(BF16)
                for n, i in enumerate(group):
                    block = values[n * slots : (n + 1) * slots]
                    target[order[i], :, :, columns] = block.reshape(inner, cap, columns.size)

            for n, piece in enumerate(pieces(other)):
                store(part_out, piece)
                for i in reversed(group):
                    j = order[i]
                    here = part_out.at[j, :, :, piece]
                    send(here, part_in.at[j, :, :, piece], 2, part_recv.at[j, n], ep, other)
            for piece in my_pieces:
                store(part_own, piece)

        def give_back(i):
            j = order[i]
            for n, piece in enumerate(my_pieces):
                arrive(part_in.at[j, :, :, piece], part_recv.at[j, n])
                total = part_own[j, :, :, piece].astype(F32) + part_in[j, :, :, piece].astype(F32)
                result[j, :, :, piece] = total.astype(BF16)
                for to in peers:
                    send(
                        result.at[j, to, :, piece],
                        back.at[j, p, :, piece],
                        3,
                        back_recv.at[j, n],
                        z * inner + to,
                        core,
                    )
                back[j, p, :, piece] = result[j, p, :, piece]

        def weigh(i):
            known = column[order[i], :, facts_at]
            chosen = dot_t(known, pick_place) == slot_of_lane
            high_part = jnp.where(chosen, dot_t(known, pick_high), 0.0).astype(BF16)
            low_part = jnp.where(chosen, dot_t(known, pick_low), 0.0).astype(BF16)
            return high_part, low_part

        def gathered(i, weights, n, piece):
            j = order[i]
            arrive(back.at[j, pl.ds(0, inner - 1), :, piece], back_recv.at[j, n])
            values = back[j, :, :, piece].reshape(slots, piece.size)
            return dot(weights[0], values) + dot(weights[1], values)

        def combine(i):
            j = order[i]
            weights = weigh(i)
            for n, piece in enumerate(my_pieces):
                sum_out[i - 1, :, piece] = gathered(i, weights, n, piece).astype(BF16)
                here = sum_out.at[i - 1, :, piece]
                send(here, sum_in.at[z, :, piece], 4, sum_recv.at[z, n], j * inner + p, core)

        def shared():
            for load in loads[5:8]:
                load.wait()
            inputs = normed[...]
            hidden = silu_product(dot(inputs, sgate_w[...]), dot(inputs, sup_w[...]))
            shared_out[:, theirs] = dot(hidden, sdown_w[:, theirs]).astype(BF16)
            here = shared_out.at[:, theirs]
            send(here, shared_in.at[:, theirs], 5, core_sem.at[0], ep, other)
            shared_out[:, mine] = dot(hidden, sdown_w[:, mine]).astype(BF16)

        def step(task, *what):
            with jax.named_scope(task.__name__ + "".join(str(w) for w in what)):
                task(*what)

        for task, *what in PLAN(outer, dispatch, shared, pair, expert, give_back, combine):
            step(task, *what)

        totals = []
        with jax.named_scope("own"):
            weights = weigh(0)
            arrive(shared_in.at[:, mine], core_sem.at[0])
            for n, piece in enumerate(my_pieces):
                shared_rows = shared_out[:, piece].astype(F32) + shared_in[:, piece].astype(F32)
                totals.append(gathered(0, weights, n, piece) + shared_rows.astype(BF16).astype(F32))
        with jax.named_scope("sums"):
            for i in range(1, outer):
                j = order[i]
                for n, piece in enumerate(my_pieces):
                    arrive(sum_in.at[j, :, piece], sum_recv.at[j, n])
                    totals[n] = totals[n] + sum_in[j, :, piece].astype(F32)
        combined = totals[0] if len(totals) == 1 else jnp.concatenate(totals, axis=1)

        lanes = last_out.shape[1] - (half - split)
        squares_at = pl.ds(half - split, lanes)
        own_squares = jnp.sum(combined * combined, axis=1, keepdims=True)
        last_out[:, squares_at] = jnp.broadcast_to(own_squares, (local_tokens, lanes))
        if core == 0:
            leaving, coming = squares_at, pl.ds(0, half - split + lanes)
        else:
            leaving, coming = pl.ds(0, half - split + lanes), squares_at
            if half > split:
                last_out[:, : half - split] = combined[:, : half - split]
        here = last_out.at[:, leaving]
        send(here, last_in.at[:, leaving], 6, core_sem.at[1], ep, other)
        with jax.named_scope("lastwait"):
            arrive(last_in.at[:, coming], core_sem.at[1])
        squares = own_squares + last_in[:, half - split : half - split + 1]
        scale = lax.rsqrt(squares / width + EPSILON)
        gain = out_gain[...].astype(F32)[None, :]
        if core == 0:
            mixed[:, :split] = (combined * scale * gain[:, :split]).astype(BF16)
            if half > split:
                extra = last_in[:, : half - split] * scale * gain[:, split:]
                mixed[:, split:] = extra.astype(BF16)
        else:
            mixed[...] = (combined[:, half - split :] * scale * gain).astype(BF16)

        for to in order[1:]:

            @pl.when(direct(to))
            def _(to=to):
                column_copy(z, to, col_send.at[to]).wait_send()

            if relay:
                on, wanted = passes(to)

                @pl.when(wanted)
                def _(to=to, on=on):
                    column_copy(to, on, col_pass.at[to]).wait_send()

        sent(staged.at[:, pl.ds(0, inner - 1), :, mine], 0)
        sent(rows_in.at[:, :, :, mine], 1)
        sent(part_out.at[:, :, :, theirs], 2)
        sent(result.at[:, pl.ds(0, inner - 1), :, mine], 3)
        sent(sum_out.at[:, :, mine], 4)
        sent(shared_out.at[:, theirs], 5)
        sent(here, 6)

    for core in range(2):

        @pl.when(tp == core)
        def _(core=core):
            on_core(core)


def plan(outer, dispatch, shared, pair, expert, give_back, combine):
    steps = [(dispatch, 0), (shared,), (dispatch, 1)]
    for i in range(2, outer):
        steps += [(pair, i - 2), (dispatch, i)]
    steps += [(pair, i) for i in range(max(0, outer - 2), 2)]
    steps += [(expert, 0, 1)]
    for i in range(2, outer):
        steps += [(pair, i)] if i >= outer - 2 else []
        steps += [(give_back, 1), (give_back, 0)] if i == 2 else [(give_back, i - 1)]
        steps += [(expert, i)]
    steps += [(combine, 1), (give_back, outer - 1)]
    steps += [(combine, i) for i in range(2, outer)]
    return steps


PLAN = plan
PIECES = (1, 2)
SPLIT = 4
RELAY = True


def body(
    experts,
    tokens,
    in_gain,
    route_expert,
    route_weight,
    gate_weight,
    up_weight,
    down_weight,
    shared_gate,
    shared_up,
    shared_down,
    out_gain,
):
    inner = 1
    while inner * inner < experts:
        inner *= 2
    outer = experts // inner
    local_tokens, width = tokens.shape
    half = width // 2
    split = width * SPLIT // 16
    top_count = route_expert.shape[1]
    capacity = max(2, (local_tokens * top_count * 4 + 3 * experts - 1) // (3 * experts))
    cap = -(-capacity // 16) * 16
    info_width = -(-3 * experts // 128) * 128
    hidden = gate_weight.shape[2]
    shared_width = shared_gate.shape[1]

    def vm(shape, kind=BF16):
        return pltpu.VMEM(shape, kind)

    grid_rows = (outer, inner, cap, width)
    most = max(PIECES)
    dma = pltpu.SemaphoreType.DMA
    in_vmem = pl.BlockSpec(memory_space=pltpu.VMEM)
    in_hbm = pl.BlockSpec(memory_space=pltpu.HBM)
    return pl.pallas_call(
        functools.partial(kernel, outer, inner, cap, info_width, split, RELAY),
        out_shape=pltpu.VMEM((local_tokens, half), BF16),
        in_specs=[in_hbm] * 11,
        out_specs=in_vmem,
        scratch_shapes=[
            vm((local_tokens, width)),
            vm((width,)),
            vm((top_count, local_tokens), jnp.int32),
            vm((top_count, local_tokens), F32),
            vm((half,)),
            vm((width, hidden)),
            vm((width, hidden)),
            vm((hidden, width)),
            vm((width, shared_width)),
            vm((width, shared_width)),
            vm((shared_width, width)),
            vm((local_tokens, width)),
            vm((outer, local_tokens, width + info_width)),
            vm(grid_rows),
            vm(grid_rows),
            vm(grid_rows),
            vm(grid_rows),
            vm(grid_rows),
            vm(grid_rows),
            vm(grid_rows),
            vm((outer - 1, local_tokens, width)),
            vm((outer, local_tokens, width)),
            vm((local_tokens, width)),
            vm((local_tokens, width)),
            vm((local_tokens, half - split + 128), F32),
            vm((local_tokens, half - split + 128), F32),
            dma((11,)),
            dma((outer,)),
            dma((outer,)),
            dma((outer,)),
            dma((outer,)),
            dma((outer,)),
            dma((outer, most)),
            dma((outer, most)),
            dma((outer, most)),
            dma((7,)),
            dma((2,)),
        ],
        compiler_params=pltpu.CompilerParams(
            collective_id=0, has_side_effects=True, vmem_limit_bytes=60 * 1024 * 1024
        ),
    )(
        tokens,
        in_gain,
        route_expert.T,
        route_weight.T,
        out_gain,
        gate_weight,
        up_weight,
        down_weight,
        shared_gate,
        shared_up,
        shared_down,
    )


def solution(mesh):
    return jax.shard_map(
        functools.partial(body, mesh.shape["ep"]),
        mesh=mesh,
        in_specs=(
            P(("grp", "ep"), None),
            P(),
            P(("grp", "ep"), None),
            P(("grp", "ep"), None),
            P("ep", None, "tp"),
            P("ep", None, "tp"),
            P("ep", "tp", None),
            P(None, "tp"),
            P(None, "tp"),
            P("tp", None),
            P("tp"),
        ),
        out_specs=P(("grp", "ep"), "tp"),
        check_vma=False,
    )
```

```python
import functools

import jax
import jax.numpy as jnp
from jax import lax
from jax.experimental import pallas as pl
from jax.experimental.pallas import tpu as pltpu
from jax.sharding import PartitionSpec as P

EPSILON = 1e-06
F32 = jnp.float32
BF16 = jnp.bfloat16


def dot(a, b):
    return jnp.dot(a, b, preferred_element_type=F32)


def dot_t(a, b):
    return lax.dot_general(a, b, (((1,), (1,)), ((), ())), preferred_element_type=F32)


def silu_product(gate_value, upward):
    return (gate_value * (1.0 / (1.0 + jnp.exp(-gate_value))) * upward).astype(BF16)


def kernel(
    outer,
    inner,
    cap,
    info_width,
    split,
    relay,
    tokens_hbm,
    in_gain_hbm,
    route_expert_hbm,
    route_weight_hbm,
    out_gain_hbm,
    gate_hbm,
    up_hbm,
    down_hbm,
    sgate_hbm,
    sup_hbm,
    sdown_hbm,
    mixed,
    tokens,
    in_gain,
    route_expert,
    route_weight,
    out_gain,
    gate_w,
    up_w,
    down_w,
    sgate_w,
    sup_w,
    sdown_w,
    normed,
    column,
    staged,
    rows_in,
    part_out,
    part_in,
    part_own,
    result,
    back,
    sum_out,
    sum_in,
    shared_out,
    shared_in,
    last_out,
    last_in,
    w_sem,
    col_send,
    col_recv,
    col_pass,
    plane_recv,
    pair_recv,
    part_recv,
    back_recv,
    sum_recv,
    send_sem,
    core_sem,
):
    ep = lax.axis_index("ep")
    tp = lax.axis_index("tp")
    z = ep // inner
    p = ep % inner
    experts = outer * inner
    local_tokens, width = tokens.shape
    half = width // 2

    loads = [
        pltpu.make_async_copy(src, dst, w_sem.at[i])
        for i, (src, dst) in enumerate(
            [
                (tokens_hbm, tokens),
                (in_gain_hbm, in_gain),
                (route_expert_hbm, route_expert),
                (route_weight_hbm, route_weight),
                (out_gain_hbm, out_gain),
                (sgate_hbm, sgate_w),
                (sup_hbm, sup_w),
                (sdown_hbm, sdown_w),
                (gate_hbm.at[0], gate_w),
                (up_hbm.at[0], up_w),
                (down_hbm.at[0], down_w),
            ]
        )
    ]
    for load in loads[:5]:
        load.start()

    barrier = pltpu.get_barrier_semaphore()

    def greet(ep_to, tp_to):
        pl.semaphore_signal(
            barrier, inc=1, device_id={"ep": ep_to, "tp": tp_to}, device_id_type=pl.DeviceIdType.MESH
        )

    for d in range(1, outer):
        greet(lax.rem(z + d, outer) * inner + p, tp)
    for d in range(1, inner):
        greet(z * inner + lax.rem(p + d, inner), tp)
    greet(ep, 1 - tp)

    for load in loads[:5]:
        load.wait()
    for load in loads[5:]:
        load.start()
    floats = tokens[...].astype(F32)
    mean = jnp.sum(floats * floats, axis=1, keepdims=True) / width
    rows = (floats * lax.rsqrt(mean + EPSILON) * in_gain[...].astype(F32)[None, :]).astype(BF16)
    normed[...] = rows

    fact = lax.broadcasted_iota(jnp.int32, (info_width, local_tokens), 0)
    fact_expert = lax.rem(fact, experts)
    named = jnp.zeros((info_width, local_tokens), F32)
    weight = jnp.zeros((info_width, local_tokens), F32)
    for k in range(route_expert.shape[0]):
        hit = route_expert[k : k + 1, :] == fact_expert
        named = named + jnp.where(hit, 1.0, 0.0)
        weight = weight + jnp.where(hit, route_weight[k : k + 1, :], 0.0)
    row_i = lax.broadcasted_iota(jnp.int32, (local_tokens, local_tokens), 0)
    col_i = lax.broadcasted_iota(jnp.int32, (local_tokens, local_tokens), 1)
    upto = jnp.where(row_i <= col_i, 1.0, 0.0).astype(BF16)
    place = dot(named.astype(BF16), upto) * named
    high = weight.astype(BF16).astype(F32)
    facts = jnp.where(fact < experts, place, jnp.where(fact < 2 * experts, high, weight - high))
    facts = jnp.where(fact < 3 * experts, facts, 0.0).astype(BF16)
    same = jnp.where(row_i == col_i, 1.0, 0.0).astype(BF16)
    info = dot_t(same, facts).astype(BF16)

    short = jnp.minimum(z, outer - 1 - z)

    def nth(i):
        if i == 0:
            return z
        near = -((i + 1) // 2) if i % 2 else i // 2
        far = jnp.where(z < outer - 1 - z, i - short, short - i)
        if i > 1:
            ends = i + 1 if i < outer - 1 else 2
            far = jnp.where(short > 0, far, jnp.where(z == 0, ends, -ends))
        return z + jnp.where(i <= 2 * short, near, far)

    order = [nth(i) for i in range(outer)]

    def direct(to):
        if not relay:
            return z >= 0
        return (to - z) * (to - z) != 4

    def passes(j):
        on = 2 * z - j
        return on, ((j - z) * (j - z) == 1) & (on >= 0) & (on < outer)

    slots = inner * cap
    slot_row = lax.broadcasted_iota(jnp.int32, (slots, info_width), 0)
    slot_lane = lax.broadcasted_iota(jnp.int32, (slots, info_width), 1)
    slot_expert = z * inner + slot_row // cap

    def selector(offset):
        return jnp.where(slot_lane == slot_expert + offset, 1.0, 0.0).astype(BF16)

    slot_rank = (lax.broadcasted_iota(jnp.int32, (slots, local_tokens), 0) % cap + 1).astype(F32)
    slot_of_lane = (lax.broadcasted_iota(jnp.int32, (local_tokens, slots), 1) % cap + 1).astype(F32)

    peers = [e + jnp.where(e < p, 0, 1) for e in range(inner - 1)]

    pl.semaphore_wait(barrier, outer + inner - 1)

    def on_core(core):
        edges = (0, split, width)
        first, end = edges[core], edges[core + 1]
        count = end - first
        other = 1 - core
        mine = pl.ds(first, count)
        theirs = pl.ds(edges[other], edges[other + 1] - edges[other])
        facts_at = pl.ds(first, info_width)
        rows_at = pl.ds(first + info_width, count)
        sent_at = pl.ds(first, info_width + count)

        def pieces(which):
            begin, stop = edges[which], edges[which + 1]
            parts = PIECES[which] if (stop - begin) % (128 * PIECES[which]) == 0 else 1
            size = (stop - begin) // parts
            return [pl.ds(begin + n * size, size) for n in range(parts)]

        my_pieces = pieces(core)

        column[z, :, facts_at] = info
        column[z, :, rows_at] = rows[:, first:end]

        def remote(src, dst, send, recv, ep_to, tp_to):
            return pltpu.make_async_remote_copy(
                src_ref=src,
                dst_ref=dst,
                send_sem=send,
                recv_sem=recv,
                device_id={"ep": ep_to, "tp": tp_to},
                device_id_type=pl.DeviceIdType.MESH,
            )

        def send(src, dst, kind, recv_sem, ep_to, tp_to):
            remote(src, dst, send_sem.at[kind], recv_sem, ep_to, tp_to).start()

        def arrive(ref, recv_sem):
            with jax.named_scope("w"):
                remote(ref, ref, send_sem.at[0], recv_sem, ep, other).wait_recv()

        def sent(ref, kind):
            remote(ref, ref, send_sem.at[kind], col_recv.at[0], ep, other).wait_send()

        def column_copy(block, to, sem):
            here = column.at[block, :, sent_at]
            return remote(here, here, sem, col_recv.at[block], to * inner + p, core)

        for to in order[1:]:

            @pl.when(direct(to))
            def _(to=to):
                column_copy(z, to, col_send.at[to]).start()

        pick_place = selector(0)
        pick_high = selector(experts)
        pick_low = selector(2 * experts)

        def dispatch(i):
            j = order[i]
            if i:
                arrive(column.at[j, :, sent_at], col_recv.at[j])
                if relay:
                    on, wanted = passes(j)

                    @pl.when(wanted)
                    def _():
                        column_copy(j, on, col_pass.at[j]).start()

            where = dot_t(pick_place, column[j, :, facts_at])
            onehot = jnp.where(where == slot_rank, 1.0, 0.0).astype(BF16)
            moved = dot(onehot, column[j, :, rows_at]).astype(BF16)
            staged[j, :, :, mine] = moved.reshape(inner, cap, count)
            for to in peers:
                send(
                    staged.at[j, to, :, mine],
                    rows_in.at[j, p, :, mine],
                    0,
                    plane_recv.at[j],
                    z * inner + to,
                    core,
                )
            rows_in[j, p, :, mine] = staged[j, p, :, mine]

        def pair(i):
            j = order[i]
            arrive(rows_in.at[j, pl.ds(0, inner - 1), :, mine], plane_recv.at[j])
            here = rows_in.at[j, :, :, mine]
            send(here, here, 1, pair_recv.at[j], ep, other)

        opened = {}

        def begin(*group):
            if group[0] == 0:
                for load in loads[8:]:
                    load.wait()

            def rows_of(columns):
                blocks = [rows_in[order[i], :, :, columns].reshape(slots, columns.size) for i in group]
                return blocks[0] if len(blocks) == 1 else jnp.concatenate(blocks, axis=0)

            own_rows = rows_of(mine)
            gate_value = dot(own_rows, gate_w[mine, :])
            upward = dot(own_rows, up_w[mine, :])
            opened[group] = gate_value, upward, rows_of

        def finish(*group):
            gate_value, upward, rows_of = opened[group]
            for i in group:
                j = order[i]
                arrive(rows_in.at[j, :, :, theirs], pair_recv.at[j])
            other_rows = rows_of(theirs)
            gate_value = gate_value + dot(other_rows, gate_w[theirs, :])
            upward = upward + dot(other_rows, up_w[theirs, :])
            opened[group] = silu_product(gate_value, upward)
            for n, piece in enumerate(pieces(other)):
                store(group, part_out, piece)
                for i in reversed(group):
                    j = order[i]
                    here = part_out.at[j, :, :, piece]
                    send(here, part_in.at[j, :, :, piece], 2, part_recv.at[j, n], ep, other)

        def settle(*group):
            for piece in my_pieces:
                store(group, part_own, piece)

        def store(group, target, columns):
            values = dot(opened[group], down_w[:, columns]).astype(BF16)
            for n, i in enumerate(group):
                block = values[n * slots : (n + 1) * slots]
                target[order[i], :, :, columns] = block.reshape(inner, cap, columns.size)

        def give_back(i):
            j = order[i]
            if i == outer - 1:
                for k in [0] + list(range(2, outer)):
                    weighed[k] = weigh(k)
            if i == 1:
                weighed[1] = weigh(1)
            for n, piece in enumerate(my_pieces):
                arrive(part_in.at[j, :, :, piece], part_recv.at[j, n])
                total = part_own[j, :, :, piece].astype(F32) + part_in[j, :, :, piece].astype(F32)
                result[j, :, :, piece] = total.astype(BF16)
                for to in peers:
                    send(
                        result.at[j, to, :, piece],
                        back.at[j, p, :, piece],
                        3,
                        back_recv.at[j, n],
                        z * inner + to,
                        core,
                    )
                back[j, p, :, piece] = result[j, p, :, piece]

        weighed = {}

        def weigh(i):
            known = column[order[i], :, facts_at]
            chosen = dot_t(known, pick_place) == slot_of_lane
            high_part = jnp.where(chosen, dot_t(known, pick_high), 0.0).astype(BF16)
            low_part = jnp.where(chosen, dot_t(known, pick_low), 0.0).astype(BF16)
            return high_part, low_part

        def gathered(i, weights, n, piece):
            j = order[i]
            arrive(back.at[j, pl.ds(0, inner - 1), :, piece], back_recv.at[j, n])
            values = back[j, :, :, piece].reshape(slots, piece.size)
            return dot(weights[0], values) + dot(weights[1], values)

        def combine(i):
            j = order[i]
            weights = weighed.pop(i)
            for n, piece in enumerate(my_pieces):
                sum_out[i - 1, :, piece] = gathered(i, weights, n, piece).astype(BF16)
                if i == outer - 1 and n == 0:

                    @pl.when(z == outer - 1)
                    def _():
                        pl.delay(DELAY)

                here = sum_out.at[i - 1, :, piece]
                send(here, sum_in.at[z, :, piece], 4, sum_recv.at[z, n], j * inner + p, core)

        def shared():
            for load in loads[5:8]:
                load.wait()
            inputs = normed[...]
            hidden = silu_product(dot(inputs, sgate_w[...]), dot(inputs, sup_w[...]))
            shared_out[:, theirs] = dot(hidden, sdown_w[:, theirs]).astype(BF16)
            here = shared_out.at[:, theirs]
            send(here, shared_in.at[:, theirs], 5, core_sem.at[0], ep, other)
            shared_out[:, mine] = dot(hidden, sdown_w[:, mine]).astype(BF16)

        def step(task, *what):
            with jax.named_scope(task.__name__ + "".join(str(w) for w in what)):
                task(*what)

        for task, *what in PLAN(outer, dispatch, shared, pair, begin, finish, settle, give_back, combine):
            step(task, *what)

        totals = []
        with jax.named_scope("own"):
            weights = weighed[0]
            arrive(shared_in.at[:, mine], core_sem.at[0])
            for n, piece in enumerate(my_pieces):
                shared_rows = shared_out[:, piece].astype(F32) + shared_in[:, piece].astype(F32)
                totals.append(gathered(0, weights, n, piece) + shared_rows.astype(BF16).astype(F32))
        with jax.named_scope("sums"):
            for i in range(1, outer):
                j = order[i]
                for n, piece in enumerate(my_pieces):
                    arrive(sum_in.at[j, :, piece], sum_recv.at[j, n])
                    totals[n] = totals[n] + sum_in[j, :, piece].astype(F32)
        combined = totals[0] if len(totals) == 1 else jnp.concatenate(totals, axis=1)

        lanes = last_out.shape[1] - (half - split)
        squares_at = pl.ds(half - split, lanes)
        own_squares = jnp.sum(combined * combined, axis=1, keepdims=True)
        last_out[:, squares_at] = jnp.broadcast_to(own_squares, (local_tokens, lanes))
        if core == 0:
            leaving, coming = squares_at, pl.ds(0, half - split + lanes)
        else:
            leaving, coming = pl.ds(0, half - split + lanes), squares_at
            if half > split:
                last_out[:, : half - split] = combined[:, : half - split]
        here = last_out.at[:, leaving]
        send(here, last_in.at[:, leaving], 6, core_sem.at[1], ep, other)
        with jax.named_scope("lastwait"):
            arrive(last_in.at[:, coming], core_sem.at[1])
        squares = own_squares + last_in[:, half - split : half - split + 1]
        scale = lax.rsqrt(squares / width + EPSILON)
        gain = out_gain[...].astype(F32)[None, :]
        if core == 0:
            mixed[:, :split] = (combined * scale * gain[:, :split]).astype(BF16)
            if half > split:
                extra = last_in[:, : half - split] * scale * gain[:, split:]
                mixed[:, split:] = extra.astype(BF16)
        else:
            mixed[...] = (combined[:, half - split :] * scale * gain).astype(BF16)

        for to in order[1:]:

            @pl.when(direct(to))
            def _(to=to):
                column_copy(z, to, col_send.at[to]).wait_send()

            if relay:
                on, wanted = passes(to)

                @pl.when(wanted)
                def _(to=to, on=on):
                    column_copy(to, on, col_pass.at[to]).wait_send()

        sent(staged.at[:, pl.ds(0, inner - 1), :, mine], 0)
        sent(rows_in.at[:, :, :, mine], 1)
        sent(part_out.at[:, :, :, theirs], 2)
        sent(result.at[:, pl.ds(0, inner - 1), :, mine], 3)
        sent(sum_out.at[:, :, mine], 4)
        sent(shared_out.at[:, theirs], 5)
        sent(here, 6)

    for core in range(2):

        @pl.when(tp == core)
        def _(core=core):
            on_core(core)


def plan(outer, dispatch, shared, pair, begin, finish, settle, give_back, combine):
    steps = [(dispatch, 0), (shared,), (dispatch, 1)]
    for i in range(2, outer):
        steps += [(pair, i - 2), (dispatch, i)]
    steps += [(pair, i) for i in range(max(0, outer - 2), 2)]
    steps += [(begin, 0, 1), (finish, 0, 1), (settle, 0, 1)]
    steps += [(pair, 2)] if 2 >= outer - 2 and outer > 2 else []
    for i in range(2, outer):
        steps += [(begin, i)]
        steps += [(give_back, 1), (give_back, 0)] if i == 2 else [(give_back, i - 1)]
        steps += [(finish, i)]
        steps += [(pair, i + 1)] if outer - 2 <= i + 1 < outer else []
        steps += [(settle, i)]
    steps += [(combine, 1), (give_back, outer - 1)]
    steps += [(combine, i) for i in range(2, outer)]
    return steps


PLAN = plan
PIECES = (1, 2)
SPLIT = 4
RELAY = True
DELAY = 1300


def body(
    experts,
    tokens,
    in_gain,
    route_expert,
    route_weight,
    gate_weight,
    up_weight,
    down_weight,
    shared_gate,
    shared_up,
    shared_down,
    out_gain,
):
    inner = 1
    while inner * inner < experts:
        inner *= 2
    outer = experts // inner
    local_tokens, width = tokens.shape
    half = width // 2
    split = width * SPLIT // 16
    top_count = route_expert.shape[1]
    capacity = max(2, (local_tokens * top_count * 4 + 3 * experts - 1) // (3 * experts))
    cap = -(-capacity // 16) * 16
    info_width = -(-3 * experts // 128) * 128
    hidden = gate_weight.shape[2]
    shared_width = shared_gate.shape[1]

    def vm(shape, kind=BF16):
        return pltpu.VMEM(shape, kind)

    grid_rows = (outer, inner, cap, width)
    most = max(PIECES)
    dma = pltpu.SemaphoreType.DMA
    in_vmem = pl.BlockSpec(memory_space=pltpu.VMEM)
    in_hbm = pl.BlockSpec(memory_space=pltpu.HBM)
    return pl.pallas_call(
        functools.partial(kernel, outer, inner, cap, info_width, split, RELAY),
        out_shape=pltpu.VMEM((local_tokens, half), BF16),
        in_specs=[in_hbm] * 11,
        out_specs=in_vmem,
        scratch_shapes=[
            vm((local_tokens, width)),
            vm((width,)),
            vm((top_count, local_tokens), jnp.int32),
            vm((top_count, local_tokens), F32),
            vm((half,)),
            vm((width, hidden)),
            vm((width, hidden)),
            vm((hidden, width)),
            vm((width, shared_width)),
            vm((width, shared_width)),
            vm((shared_width, width)),
            vm((local_tokens, width)),
            vm((outer, local_tokens, width + info_width)),
            vm(grid_rows),
            vm(grid_rows),
            vm(grid_rows),
            vm(grid_rows),
            vm(grid_rows),
            vm(grid_rows),
            vm(grid_rows),
            vm((outer - 1, local_tokens, width)),
            vm((outer, local_tokens, width)),
            vm((local_tokens, width)),
            vm((local_tokens, width)),
            vm((local_tokens, half - split + 128), F32),
            vm((local_tokens, half - split + 128), F32),
            dma((11,)),
            dma((outer,)),
            dma((outer,)),
            dma((outer,)),
            dma((outer,)),
            dma((outer,)),
            dma((outer, most)),
            dma((outer, most)),
            dma((outer, most)),
            dma((7,)),
            dma((2,)),
        ],
        compiler_params=pltpu.CompilerParams(
            collective_id=0, has_side_effects=True, vmem_limit_bytes=60 * 1024 * 1024
        ),
    )(
        tokens,
        in_gain,
        route_expert.T,
        route_weight.T,
        out_gain,
        gate_weight,
        up_weight,
        down_weight,
        shared_gate,
        shared_up,
        shared_down,
    )


def solution(mesh):
    return jax.shard_map(
        functools.partial(body, mesh.shape["ep"]),
        mesh=mesh,
        in_specs=(
            P(("grp", "ep"), None),
            P(),
            P(("grp", "ep"), None),
            P(("grp", "ep"), None),
            P("ep", None, "tp"),
            P("ep", None, "tp"),
            P("ep", "tp", None),
            P(None, "tp"),
            P(None, "tp"),
            P("tp", None),
            P("tp"),
        ),
        out_specs=P(("grp", "ep"), "tp"),
        check_vma=False,
    )
```

```python
import functools

import jax
import jax.numpy as jnp
from jax import lax
from jax.experimental import pallas as pl
from jax.experimental.pallas import tpu as pltpu
from jax.sharding import PartitionSpec as P

EPSILON = 1e-06
F32 = jnp.float32
BF16 = jnp.bfloat16


def dot(a, b):
    return jnp.dot(a, b, preferred_element_type=F32)


def dot_t(a, b):
    return lax.dot_general(a, b, (((1,), (1,)), ((), ())), preferred_element_type=F32)


def silu_product(gate_value, upward):
    return (gate_value * (1.0 / (1.0 + jnp.exp(-gate_value))) * upward).astype(BF16)


def kernel(
    outer,
    inner,
    cap,
    info_width,
    split,
    relay,
    tokens_hbm,
    in_gain_hbm,
    route_expert_hbm,
    route_weight_hbm,
    out_gain_hbm,
    gate_hbm,
    up_hbm,
    down_hbm,
    sgate_hbm,
    sup_hbm,
    sdown_hbm,
    mixed,
    tokens,
    in_gain,
    route_expert,
    route_weight,
    out_gain,
    gate_w,
    up_w,
    down_w,
    sgate_w,
    sup_w,
    sdown_w,
    normed,
    column,
    staged,
    rows_in,
    part_out,
    part_in,
    part_own,
    result,
    back,
    sum_out,
    sum_in,
    shared_out,
    shared_in,
    last_out,
    last_in,
    w_sem,
    col_send,
    col_recv,
    col_pass,
    plane_recv,
    pair_recv,
    part_recv,
    back_recv,
    sum_recv,
    send_sem,
    core_sem,
):
    ep = lax.axis_index("ep")
    tp = lax.axis_index("tp")
    z = ep // inner
    p = ep % inner
    experts = outer * inner
    local_tokens, width = tokens.shape
    half = width // 2

    loads = [
        pltpu.make_async_copy(src, dst, w_sem.at[i])
        for i, (src, dst) in enumerate(
            [
                (tokens_hbm, tokens),
                (in_gain_hbm, in_gain),
                (route_expert_hbm, route_expert),
                (route_weight_hbm, route_weight),
                (out_gain_hbm, out_gain),
                (sgate_hbm, sgate_w),
                (sup_hbm, sup_w),
                (sdown_hbm, sdown_w),
                (gate_hbm.at[0], gate_w),
                (up_hbm.at[0], up_w),
                (down_hbm.at[0], down_w),
            ]
        )
    ]
    for load in loads[:5]:
        load.start()

    barrier = pltpu.get_barrier_semaphore()

    def greet(ep_to, tp_to):
        pl.semaphore_signal(
            barrier, inc=1, device_id={"ep": ep_to, "tp": tp_to}, device_id_type=pl.DeviceIdType.MESH
        )

    for d in range(1, outer):
        greet(lax.rem(z + d, outer) * inner + p, tp)
    for d in range(1, inner):
        greet(z * inner + lax.rem(p + d, inner), tp)
    greet(ep, 1 - tp)

    for load in loads[:5]:
        load.wait()
    for load in loads[5:]:
        load.start()
    floats = tokens[...].astype(F32)
    mean = jnp.sum(floats * floats, axis=1, keepdims=True) / width
    rows = (floats * lax.rsqrt(mean + EPSILON) * in_gain[...].astype(F32)[None, :]).astype(BF16)
    normed[...] = rows

    fact = lax.broadcasted_iota(jnp.int32, (info_width, local_tokens), 0)
    fact_expert = lax.rem(fact, experts)
    named = jnp.zeros((info_width, local_tokens), F32)
    weight = jnp.zeros((info_width, local_tokens), F32)
    for k in range(route_expert.shape[0]):
        hit = route_expert[k : k + 1, :] == fact_expert
        named = named + jnp.where(hit, 1.0, 0.0)
        weight = weight + jnp.where(hit, route_weight[k : k + 1, :], 0.0)
    row_i = lax.broadcasted_iota(jnp.int32, (local_tokens, local_tokens), 0)
    col_i = lax.broadcasted_iota(jnp.int32, (local_tokens, local_tokens), 1)
    upto = jnp.where(row_i <= col_i, 1.0, 0.0).astype(BF16)
    place = dot(named.astype(BF16), upto) * named
    high = weight.astype(BF16).astype(F32)
    facts = jnp.where(fact < experts, place, jnp.where(fact < 2 * experts, high, weight - high))
    facts = jnp.where(fact < 3 * experts, facts, 0.0).astype(BF16)
    same = jnp.where(row_i == col_i, 1.0, 0.0).astype(BF16)
    info = dot_t(same, facts).astype(BF16)

    short = jnp.minimum(z, outer - 1 - z)

    def nth(i):
        if i == 0:
            return z
        near = -((i + 1) // 2) if i % 2 else i // 2
        far = jnp.where(z < outer - 1 - z, i - short, short - i)
        if i > 1:
            ends = i + 1 if i < outer - 1 else 2
            far = jnp.where(short > 0, far, jnp.where(z == 0, ends, -ends))
        return z + jnp.where(i <= 2 * short, near, far)

    order = [nth(i) for i in range(outer)]

    def direct(to):
        if not relay:
            return z >= 0
        return (to - z) * (to - z) != 4

    def passes(j):
        on = 2 * z - j
        return on, ((j - z) * (j - z) == 1) & (on >= 0) & (on < outer)

    slots = inner * cap
    slot_row = lax.broadcasted_iota(jnp.int32, (slots, info_width), 0)
    slot_lane = lax.broadcasted_iota(jnp.int32, (slots, info_width), 1)
    slot_expert = z * inner + slot_row // cap

    def selector(offset):
        return jnp.where(slot_lane == slot_expert + offset, 1.0, 0.0).astype(BF16)

    slot_rank = (lax.broadcasted_iota(jnp.int32, (slots, local_tokens), 0) % cap + 1).astype(F32)
    slot_of_lane = (lax.broadcasted_iota(jnp.int32, (local_tokens, slots), 1) % cap + 1).astype(F32)

    peers = [e + jnp.where(e < p, 0, 1) for e in range(inner - 1)]


    def on_core(core):
        edges = (0, split, width)
        first, end = edges[core], edges[core + 1]
        count = end - first
        other = 1 - core
        mine = pl.ds(first, count)
        theirs = pl.ds(edges[other], edges[other + 1] - edges[other])
        kept = pl.ds(core * half, half)
        given = pl.ds(other * half, half)
        facts_at = pl.ds(first, info_width)
        rows_at = pl.ds(first + info_width, count)
        sent_at = pl.ds(first, info_width + count)

        def pieces(which):
            if which == 0:
                return [pl.ds(0, split)]
            return [pl.ds(split, half - split), pl.ds(half, half)]

        my_pieces = pieces(core)
        pl.semaphore_wait(barrier, outer + inner - 1)

        column[z, :, facts_at] = info
        column[z, :, rows_at] = rows[:, first:end]

        def remote(src, dst, send, recv, ep_to, tp_to):
            return pltpu.make_async_remote_copy(
                src_ref=src,
                dst_ref=dst,
                send_sem=send,
                recv_sem=recv,
                device_id={"ep": ep_to, "tp": tp_to},
                device_id_type=pl.DeviceIdType.MESH,
            )

        def send(src, dst, kind, recv_sem, ep_to, tp_to):
            remote(src, dst, send_sem.at[kind], recv_sem, ep_to, tp_to).start()

        def arrive(ref, recv_sem):
            with jax.named_scope("w"):
                remote(ref, ref, send_sem.at[0], recv_sem, ep, other).wait_recv()

        def sent(ref, kind):
            remote(ref, ref, send_sem.at[kind], col_recv.at[0], ep, other).wait_send()

        def column_copy(block, to, sem):
            here = column.at[block, :, sent_at]
            return remote(here, here, sem, col_recv.at[block], to * inner + p, core)

        for to in order[1:]:

            @pl.when(direct(to))
            def _(to=to):
                column_copy(z, to, col_send.at[to]).start()

        pick_place = selector(0)
        pick_high = selector(experts)
        pick_low = selector(2 * experts)

        def dispatch(i):
            j = order[i]
            if i:
                arrive(column.at[j, :, sent_at], col_recv.at[j])
                if relay:
                    on, wanted = passes(j)

                    @pl.when(wanted)
                    def _():
                        column_copy(j, on, col_pass.at[j]).start()

            where = dot_t(pick_place, column[j, :, facts_at])
            onehot = jnp.where(where == slot_rank, 1.0, 0.0).astype(BF16)
            moved = dot(onehot, column[j, :, rows_at]).astype(BF16)
            staged[j, :, :, mine] = moved.reshape(inner, cap, count)
            for to in peers:
                send(
                    staged.at[j, to, :, mine],
                    rows_in.at[j, p, :, mine],
                    0,
                    plane_recv.at[j],
                    z * inner + to,
                    core,
                )
            rows_in[j, p, :, mine] = staged[j, p, :, mine]

        def pair(i):
            j = order[i]
            arrive(rows_in.at[j, pl.ds(0, inner - 1), :, mine], plane_recv.at[j])
            here = rows_in.at[j, :, :, mine]
            send(here, here, 1, pair_recv.at[j], ep, other)

        opened = {}

        def begin(*group):
            if group[0] == 0:
                for load in loads[8:]:
                    load.wait()

            def rows_of(columns):
                blocks = [rows_in[order[i], :, :, columns].reshape(slots, columns.size) for i in group]
                return blocks[0] if len(blocks) == 1 else jnp.concatenate(blocks, axis=0)

            own_rows = rows_of(mine)
            gate_value = dot(own_rows, gate_w[mine, :])
            upward = dot(own_rows, up_w[mine, :])
            opened[group] = gate_value, upward, rows_of

        def finish(*group):
            gate_value, upward, rows_of = opened[group]
            for i in group:
                j = order[i]
                arrive(rows_in.at[j, :, :, theirs], pair_recv.at[j])
            other_rows = rows_of(theirs)
            gate_value = gate_value + dot(other_rows, gate_w[theirs, :])
            upward = upward + dot(other_rows, up_w[theirs, :])
            if len(group) == 1 and outer - 2 <= group[0] + 1 < outer:
                pair(group[0] + 1)
            opened[group] = silu_product(gate_value, upward)
            for n, piece in enumerate(pieces(other)):
                store(group, part_out, piece)
                for i in reversed(group):
                    j = order[i]
                    here = part_out.at[j, :, :, piece]
                    send(here, part_in.at[j, :, :, piece], 2, part_recv.at[j, n], ep, other)

        def settle(*group):
            for piece in my_pieces:
                store(group, part_own, piece)

        def store(group, target, columns):
            values = dot(opened[group], down_w[:, columns]).astype(BF16)
            for n, i in enumerate(group):
                block = values[n * slots : (n + 1) * slots]
                target[order[i], :, :, columns] = block.reshape(inner, cap, columns.size)

        def give_back(i):
            j = order[i]
            if i == outer - 1:
                for k in [0] + list(range(2, outer)):
                    weighed[k] = weigh(k)
            if i == 1:
                weighed[1] = weigh(1)
            for n, piece in enumerate(my_pieces):
                arrive(part_in.at[j, :, :, piece], part_recv.at[j, n])
                total = part_own[j, :, :, piece].astype(F32) + part_in[j, :, :, piece].astype(F32)
                result[j, :, :, piece] = total.astype(BF16)
                for to in peers:
                    send(
                        result.at[j, to, :, piece],
                        back.at[j, p, :, piece],
                        3,
                        back_recv.at[j, n],
                        z * inner + to,
                        core,
                    )
                back[j, p, :, piece] = result[j, p, :, piece]

        weighed = {}

        def weigh(i):
            known = column[order[i], :, facts_at]
            chosen = dot_t(known, pick_place) == slot_of_lane
            high_part = jnp.where(chosen, dot_t(known, pick_high), 0.0).astype(BF16)
            low_part = jnp.where(chosen, dot_t(known, pick_low), 0.0).astype(BF16)
            return jnp.concatenate([high_part, low_part], axis=0)

        def gathered(i, weights, n, piece):
            j = order[i]
            arrive(back.at[j, pl.ds(0, inner - 1), :, piece], back_recv.at[j, n])
            values = back[j, :, :, piece].reshape(slots, piece.size)
            both = dot(weights, values)
            return both[:local_tokens] + both[local_tokens:]

        def combine(i):
            j = order[i]
            weights = weighed.pop(i)
            for n, piece in enumerate(my_pieces):
                sum_out[i - 1, :, piece] = gathered(i, weights, n, piece).astype(BF16)
                if i == outer - 1 and n == 0:

                    for end, cycles in ((0, DELAY[0]), (outer - 1, DELAY[1])):

                        @pl.when(z == end)
                        def _(cycles=cycles):
                            pl.delay(cycles)

                here = sum_out.at[i - 1, :, piece]
                lower = core - core * n
                send(here, sum_in.at[z, :, piece], 4, sum_recv.at[z, lower], j * inner + p, core * n)

        def shared():
            for load in loads[5:8]:
                load.wait()
            inputs = normed[...]
            hidden = silu_product(dot(inputs, sgate_w[...]), dot(inputs, sup_w[...]))
            shared_out[:, given] = dot(hidden, sdown_w[:, given]).astype(BF16)
            here = shared_out.at[:, given]
            send(here, shared_in.at[:, given], 5, core_sem.at[0], ep, other)
            shared_out[:, kept] = dot(hidden, sdown_w[:, kept]).astype(BF16)

        def step(task, *what):
            with jax.named_scope(task.__name__ + "".join(str(w) for w in what)):
                task(*what)

        for task, *what in PLAN(core, outer, dispatch, shared, pair, begin, finish, settle, give_back, combine):
            step(task, *what)

        with jax.named_scope("own"):
            weights = weighed[0]
            mixed_rows = [gathered(0, weights, n, piece) for n, piece in enumerate(my_pieces)]
            lent = pl.ds(split, half - split)
            if core == 1:
                sum_out[outer - 1, :, lent] = mixed_rows[0].astype(BF16)
                here = sum_out.at[outer - 1, :, lent]
                send(here, sum_in.at[z, :, lent], 7, sum_recv.at[z, 1], ep, 0)
            owned = [(my_pieces[core], 0)]
            arrive(shared_in.at[:, kept], core_sem.at[0])
            shared_rows = shared_out[:, kept].astype(F32) + shared_in[:, kept].astype(F32)
            shared_rows = shared_rows.astype(BF16).astype(F32)
            totals = [mixed_rows[core] + shared_rows[:, : my_pieces[core].size]]
            if core == 0:
                arrive(sum_in.at[z, :, lent], sum_recv.at[z, 1])
                totals.append(shared_rows[:, split:] + sum_in[z, :, lent].astype(F32))
                owned.append((lent, 1))
        with jax.named_scope("sums"):
            for i in range(1, outer):
                j = order[i]
                for k, (piece, n) in enumerate(owned):
                    arrive(sum_in.at[j, :, piece], sum_recv.at[j, n])
                    totals[k] = totals[k] + sum_in[j, :, piece].astype(F32)
        combined = totals[0] if len(totals) == 1 else jnp.concatenate(totals, axis=1)

        own_squares = jnp.sum(combined * combined, axis=1, keepdims=True)
        last_out[...] = jnp.broadcast_to(own_squares, last_out.shape)
        send(last_out, last_in, 6, core_sem.at[1], ep, other)
        scaled = combined * out_gain[...].astype(F32)[None, :]
        with jax.named_scope("lastwait"):
            arrive(last_in, core_sem.at[1])
        squares = own_squares + last_in[:, :1]
        mixed[...] = (scaled * lax.rsqrt(squares / width + EPSILON)).astype(BF16)

        for to in order[1:]:

            @pl.when(direct(to))
            def _(to=to):
                column_copy(z, to, col_send.at[to]).wait_send()

            if relay:
                on, wanted = passes(to)

                @pl.when(wanted)
                def _(to=to, on=on):
                    column_copy(to, on, col_pass.at[to]).wait_send()

        sent(staged.at[:, pl.ds(0, inner - 1), :, mine], 0)
        sent(rows_in.at[:, :, :, mine], 1)
        sent(part_out.at[:, :, :, theirs], 2)
        sent(result.at[:, pl.ds(0, inner - 1), :, mine], 3)
        sent(sum_out.at[pl.ds(0, outer - 1), :, mine], 4)
        sent(shared_out.at[:, given], 5)
        sent(last_out, 6)
        if core == 1:
            sent(sum_out.at[outer - 1, :, lent], 7)

    for core in range(2):

        @pl.when(tp == core)
        def _(core=core):
            on_core(core)


def plan(core, outer, dispatch, shared, pair, begin, finish, settle, give_back, combine):
    steps = [(dispatch, 0), (shared,), (dispatch, 1)]
    for i in range(2, outer):
        steps += [(pair, i - 2), (dispatch, i)]
    steps += [(pair, i) for i in range(max(0, outer - 2), 2)]
    steps += [(begin, 0, 1), (finish, 0, 1), (settle, 0, 1)]
    steps += [(pair, 2)] if 2 >= outer - 2 and outer > 2 else []
    for i in range(2, outer):
        earlier = [(give_back, 1), (give_back, 0)] if i == 2 else [(give_back, i - 1)]
        steps += [(begin, i)]
        steps += [(finish, i)] + earlier if core and i > 2 else earlier + [(finish, i)]
        steps += [(settle, i)]
    steps += [(give_back, outer - 1)]
    steps += [(combine, i) for i in range(1, outer)]
    return steps


PLAN = plan
SPLIT = 2
RELAY = True
DELAY = (0, 1300)


def body(
    experts,
    tokens,
    in_gain,
    route_expert,
    route_weight,
    gate_weight,
    up_weight,
    down_weight,
    shared_gate,
    shared_up,
    shared_down,
    out_gain,
):
    inner = 1
    while inner * inner < experts:
        inner *= 2
    outer = experts // inner
    local_tokens, width = tokens.shape
    half = width // 2
    split = width * SPLIT // 16
    top_count = route_expert.shape[1]
    capacity = max(2, (local_tokens * top_count * 4 + 3 * experts - 1) // (3 * experts))
    cap = -(-capacity // 16) * 16
    info_width = -(-3 * experts // 128) * 128
    hidden = gate_weight.shape[2]
    shared_width = shared_gate.shape[1]

    def vm(shape, kind=BF16):
        return pltpu.VMEM(shape, kind)

    grid_rows = (outer, inner, cap, width)
    most = 2
    dma = pltpu.SemaphoreType.DMA
    in_vmem = pl.BlockSpec(memory_space=pltpu.VMEM)
    in_hbm = pl.BlockSpec(memory_space=pltpu.HBM)
    return pl.pallas_call(
        functools.partial(kernel, outer, inner, cap, info_width, split, RELAY),
        out_shape=pltpu.VMEM((local_tokens, half), BF16),
        in_specs=[in_hbm] * 11,
        out_specs=in_vmem,
        scratch_shapes=[
            vm((local_tokens, width)),
            vm((width,)),
            vm((top_count, local_tokens), jnp.int32),
            vm((top_count, local_tokens), F32),
            vm((half,)),
            vm((width, hidden)),
            vm((width, hidden)),
            vm((hidden, width)),
            vm((width, shared_width)),
            vm((width, shared_width)),
            vm((shared_width, width)),
            vm((local_tokens, width)),
            vm((outer, local_tokens, width + info_width)),
            vm(grid_rows),
            vm(grid_rows),
            vm(grid_rows),
            vm(grid_rows),
            vm(grid_rows),
            vm(grid_rows),
            vm(grid_rows),
            vm((outer, local_tokens, width)),
            vm((outer, local_tokens, width)),
            vm((local_tokens, width)),
            vm((local_tokens, width)),
            vm((local_tokens, 128), F32),
            vm((local_tokens, 128), F32),
            dma((11,)),
            dma((outer,)),
            dma((outer,)),
            dma((outer,)),
            dma((outer,)),
            dma((outer,)),
            dma((outer, most)),
            dma((outer, most)),
            dma((outer, most)),
            dma((8,)),
            dma((2,)),
        ],
        compiler_params=pltpu.CompilerParams(
            collective_id=0, has_side_effects=True, vmem_limit_bytes=60 * 1024 * 1024
        ),
    )(
        tokens,
        in_gain,
        route_expert.T,
        route_weight.T,
        out_gain,
        gate_weight,
        up_weight,
        down_weight,
        shared_gate,
        shared_up,
        shared_down,
    )


def solution(mesh):
    return jax.shard_map(
        functools.partial(body, mesh.shape["ep"]),
        mesh=mesh,
        in_specs=(
            P(("grp", "ep"), None),
            P(),
            P(("grp", "ep"), None),
            P(("grp", "ep"), None),
            P("ep", None, "tp"),
            P("ep", None, "tp"),
            P("ep", "tp", None),
            P(None, "tp"),
            P(None, "tp"),
            P("tp", None),
            P("tp"),
        ),
        out_specs=P(("grp", "ep"), "tp"),
        check_vma=False,
    )
```

```python
import functools

import jax
import jax.numpy as jnp
from jax import lax
from jax.experimental import pallas as pl
from jax.experimental.pallas import tpu as pltpu
from jax.sharding import PartitionSpec as P

EPSILON = 1e-06
F32 = jnp.float32
BF16 = jnp.bfloat16


def dot(a, b):
    return jnp.dot(a, b, preferred_element_type=F32)


def dot_t(a, b):
    return lax.dot_general(a, b, (((1,), (1,)), ((), ())), preferred_element_type=F32)


def silu_product(gate_value, upward):
    return (gate_value * (1.0 / (1.0 + jnp.exp(-gate_value))) * upward).astype(BF16)


def column_sends(outer):
    counts = []
    for z in range(outer):
        straight = [j for j in range(outer) if j != z and (z == 0 or abs(j - z) != 2)]
        passed = [j for j in (z - 1, z + 1) if 0 < j < outer and 0 <= 2 * z - j < outer]
        counts.append(len(straight) + len(passed))
    return counts


def kernel(
    outer,
    inner,
    cap,
    info_width,
    split,
    tokens_hbm,
    in_gain_hbm,
    route_expert_hbm,
    route_weight_hbm,
    out_gain_hbm,
    gate_hbm,
    up_hbm,
    down_hbm,
    sgate_hbm,
    sup_hbm,
    sdown_hbm,
    mixed,
    tokens,
    in_gain,
    route_expert,
    route_weight,
    out_gain,
    gate_w,
    up_w,
    down_w,
    sgate_w,
    sup_w,
    sdown_w,
    normed,
    column,
    staged,
    rows_in,
    part_out,
    part_in,
    part_own,
    result,
    back,
    sum_out,
    sum_in,
    shared_out,
    shared_in,
    last_out,
    last_in,
    w_sem,
    col_recv,
    plane_recv,
    pair_recv,
    part_recv,
    back_recv,
    sum_recv,
    send_sem,
    core_sem,
):
    ep = lax.axis_index("ep")
    tp = lax.axis_index("tp")
    z = ep // inner
    p = ep % inner
    experts = outer * inner
    local_tokens, width = tokens.shape
    half = width // 2

    loads = [
        pltpu.make_async_copy(src, dst, w_sem.at[i])
        for i, (src, dst) in enumerate(
            [
                (tokens_hbm, tokens),
                (in_gain_hbm, in_gain),
                (route_expert_hbm, route_expert),
                (route_weight_hbm, route_weight),
                (out_gain_hbm, out_gain),
                (sgate_hbm, sgate_w),
                (sup_hbm, sup_w),
                (sdown_hbm, sdown_w),
                (gate_hbm.at[0], gate_w),
                (up_hbm.at[0], up_w),
                (down_hbm.at[0], down_w),
            ]
        )
    ]
    for load in loads[:5]:
        load.start()

    barrier = pltpu.get_barrier_semaphore()

    def greet(ep_to, tp_to):
        pl.semaphore_signal(
            barrier, inc=1, device_id={"ep": ep_to, "tp": tp_to}, device_id_type=pl.DeviceIdType.MESH
        )

    for d in range(1, outer):
        greet(lax.rem(z + d, outer) * inner + p, tp)
    for d in range(1, inner):
        greet(z * inner + lax.rem(p + d, inner), tp)
    greet(ep, 1 - tp)

    for load in loads[:5]:
        load.wait()
    for load in loads[5:]:
        load.start()
    floats = tokens[...].astype(F32)
    mean = jnp.sum(floats * floats, axis=1, keepdims=True) / width
    rows = (floats * lax.rsqrt(mean + EPSILON) * in_gain[...].astype(F32)[None, :]).astype(BF16)
    normed[...] = rows

    fact = lax.broadcasted_iota(jnp.int32, (info_width, local_tokens), 0)
    fact_expert = lax.rem(fact, experts)
    named = jnp.zeros((info_width, local_tokens), F32)
    weight = jnp.zeros((info_width, local_tokens), F32)
    for k in range(route_expert.shape[0]):
        hit = route_expert[k : k + 1, :] == fact_expert
        named = named + jnp.where(hit, 1.0, 0.0)
        weight = weight + jnp.where(hit, route_weight[k : k + 1, :], 0.0)
    row_i = lax.broadcasted_iota(jnp.int32, (local_tokens, local_tokens), 0)
    col_i = lax.broadcasted_iota(jnp.int32, (local_tokens, local_tokens), 1)
    upto = jnp.where(row_i <= col_i, 1.0, 0.0).astype(BF16)
    place = dot(named.astype(BF16), upto) * named
    high = weight.astype(BF16).astype(F32)
    facts = jnp.where(fact < experts, place, jnp.where(fact < 2 * experts, high, weight - high))
    facts = jnp.where(fact < 3 * experts, facts, 0.0).astype(BF16)
    same = jnp.where(row_i == col_i, 1.0, 0.0).astype(BF16)
    info = dot_t(same, facts).astype(BF16)

    short = jnp.minimum(z, outer - 1 - z)

    def nth(i):
        if i == 0:
            return z
        near = -((i + 1) // 2) if i % 2 else i // 2
        far = jnp.where(z < outer - 1 - z, i - short, short - i)
        if i > 1:
            ends = i + 1 if i < outer - 1 else 2
            far = jnp.where(short > 0, far, jnp.where(z == 0, ends, -ends))
        return z + jnp.where(i <= 2 * short, near, far)

    order = [nth(i) for i in range(outer)]
    passing = list(order)
    if outer > 3:
        swap = z == outer - 2
        passing[-2:] = [jnp.where(swap, order[-1], order[-2]), jnp.where(swap, order[-2], order[-1])]

    def direct(to):
        return (z == 0) | ((to - z) * (to - z) != 4)

    def passes(j):
        on = 2 * z - j
        return on, ((j - z) * (j - z) == 1) & (on >= 0) & (on < outer) & (j > 0)

    slots = inner * cap
    slot_row = lax.broadcasted_iota(jnp.int32, (slots, info_width), 0)
    slot_lane = lax.broadcasted_iota(jnp.int32, (slots, info_width), 1)
    slot_expert = z * inner + slot_row // cap

    def selector(offset):
        return jnp.where(slot_lane == slot_expert + offset, 1.0, 0.0).astype(BF16)

    slot_rank = (lax.broadcasted_iota(jnp.int32, (slots, local_tokens), 0) % cap + 1).astype(F32)
    slot_of_lane = (lax.broadcasted_iota(jnp.int32, (local_tokens, slots), 1) % cap + 1).astype(F32)

    peers = [e + jnp.where(e < p, 0, 1) for e in range(inner - 1)]


    def on_core(core):
        edges = (0, split, width)
        first, end = edges[core], edges[core + 1]
        count = end - first
        other = 1 - core
        mine = pl.ds(first, count)
        theirs = pl.ds(edges[other], edges[other + 1] - edges[other])
        kept = pl.ds(core * half, half)
        given = pl.ds(other * half, half)
        facts_at = pl.ds(first, info_width)
        rows_at = pl.ds(first + info_width, count)
        sent_at = pl.ds(first, info_width + count)

        def pieces(which):
            if which == 0:
                return [pl.ds(0, split)]
            return [pl.ds(split, half - split), pl.ds(half, half)]

        my_pieces = pieces(core)
        pl.semaphore_wait(barrier, outer + inner - 1)

        column[z, :, facts_at] = info
        column[z, :, rows_at] = rows[:, first:end]

        def remote(src, dst, send, recv, ep_to, tp_to):
            return pltpu.make_async_remote_copy(
                src_ref=src,
                dst_ref=dst,
                send_sem=send,
                recv_sem=recv,
                device_id={"ep": ep_to, "tp": tp_to},
                device_id_type=pl.DeviceIdType.MESH,
            )

        def send(src, dst, kind, recv_sem, ep_to, tp_to):
            remote(src, dst, send_sem.at[kind], recv_sem, ep_to, tp_to).start()

        def arrive(ref, recv_sem):
            with jax.named_scope("w"):
                remote(ref, ref, send_sem.at[0], recv_sem, ep, other).wait_recv()

        def sent(ref, kind):
            remote(ref, ref, send_sem.at[kind], col_recv.at[0], ep, other).wait_send()

        def column_copy(block, to):
            here = column.at[block, :, sent_at]
            return remote(here, here, send_sem.at[8], col_recv.at[block], to * inner + p, core)

        for i, to in enumerate(order[1:], 1):
            to = jnp.where(z == 0, i, to)

            @pl.when(direct(to))
            def _(to=to):
                column_copy(z, to).start()

        pick_place = selector(0)
        pick_high = selector(experts)
        pick_low = selector(2 * experts)

        def dispatch(i, early=None):
            if i < outer - 1 or i == 1:
                move(i)
            else:

                @pl.when((z == outer - 2) == early)
                def _():
                    move(i)

        def move(i):
            j = order[i]
            if i:
                arrive(column.at[j, :, sent_at], col_recv.at[j])
                on, wanted = passes(j)

                @pl.when(wanted)
                def _():
                    column_copy(j, on).start()

            where = dot_t(pick_place, column[j, :, facts_at])
            onehot = jnp.where(where == slot_rank, 1.0, 0.0).astype(BF16)
            moved = dot(onehot, column[j, :, rows_at]).astype(BF16)
            staged[j, :, :, mine] = moved.reshape(inner, cap, count)
            for to in peers:
                send(
                    staged.at[j, to, :, mine],
                    rows_in.at[j, p, :, mine],
                    0,
                    plane_recv.at[j],
                    z * inner + to,
                    core,
                )
            rows_in[j, p, :, mine] = staged[j, p, :, mine]

        def pair(i):
            j = passing[i]
            arrive(rows_in.at[j, pl.ds(0, inner - 1), :, mine], plane_recv.at[j])
            here = rows_in.at[j, :, :, mine]
            send(here, here, 1, pair_recv.at[j], ep, other)

        opened = {}

        def begin(*group):
            if group[0] == 0:
                for load in loads[8:]:
                    load.wait()

            def rows_of(columns):
                blocks = [rows_in[passing[i], :, :, columns].reshape(slots, columns.size) for i in group]
                return blocks[0] if len(blocks) == 1 else jnp.concatenate(blocks, axis=0)

            own_rows = rows_of(mine)
            gate_value = dot(own_rows, gate_w[mine, :])
            upward = dot(own_rows, up_w[mine, :])
            opened[group] = gate_value, upward, rows_of

        def finish(*group):
            gate_value, upward, rows_of = opened[group]
            for i in group:
                j = passing[i]
                arrive(rows_in.at[j, :, :, theirs], pair_recv.at[j])
            other_rows = rows_of(theirs)
            gate_value = gate_value + dot(other_rows, gate_w[theirs, :])
            upward = upward + dot(other_rows, up_w[theirs, :])
            if len(group) == 1 and outer - 2 <= group[0] + 1 < outer:
                pair(group[0] + 1)
            opened[group] = silu_product(gate_value, upward)
            for n, piece in enumerate(pieces(other)):
                store(group, part_out, piece)
                for i in reversed(group):
                    j = passing[i]
                    here = part_out.at[j, :, :, piece]
                    send(here, part_in.at[j, :, :, piece], 2, part_recv.at[j, n], ep, other)

        def settle(*group):
            for piece in my_pieces:
                store(group, part_own, piece)

        def store(group, target, columns):
            values = dot(opened[group], down_w[:, columns]).astype(BF16)
            for n, i in enumerate(group):
                block = values[n * slots : (n + 1) * slots]
                target[passing[i], :, :, columns] = block.reshape(inner, cap, columns.size)

        def give_back(i):
            j = passing[i]
            if i == outer - 1:
                for k in [0] + list(range(2, outer)):
                    weighed[k] = weigh(k)
            if i == 1:
                weighed[1] = weigh(1)
            for n, piece in enumerate(my_pieces):
                arrive(part_in.at[j, :, :, piece], part_recv.at[j, n])
                total = part_own[j, :, :, piece].astype(F32) + part_in[j, :, :, piece].astype(F32)
                result[j, :, :, piece] = total.astype(BF16)
                for to in peers:
                    send(
                        result.at[j, to, :, piece],
                        back.at[j, p, :, piece],
                        3,
                        back_recv.at[j, n],
                        z * inner + to,
                        core,
                    )
                back[j, p, :, piece] = result[j, p, :, piece]

        weighed = {}

        def weigh(i):
            known = column[passing[i], :, facts_at]
            chosen = dot_t(known, pick_place) == slot_of_lane
            high_part = jnp.where(chosen, dot_t(known, pick_high), 0.0).astype(BF16)
            low_part = jnp.where(chosen, dot_t(known, pick_low), 0.0).astype(BF16)
            return jnp.concatenate([high_part, low_part], axis=0)

        def gathered(i, weights, n, piece):
            j = passing[i]
            arrive(back.at[j, pl.ds(0, inner - 1), :, piece], back_recv.at[j, n])
            values = back[j, :, :, piece].reshape(slots, piece.size)
            both = dot(weights, values)
            return both[:local_tokens] + both[local_tokens:]

        def combine(i):
            j = passing[i]
            weights = weighed.pop(i)
            for n, piece in enumerate(my_pieces):
                sum_out[i - 1, :, piece] = gathered(i, weights, n, piece).astype(BF16)
                if i == outer - 1 and n == 0:

                    for end, cycles in ((0, DELAY[0]), (outer - 1, DELAY[1])):

                        @pl.when(z == end)
                        def _(cycles=cycles):
                            pl.delay(cycles)

                here = sum_out.at[i - 1, :, piece]
                lower = core - core * n
                send(here, sum_in.at[z, :, piece], 4, sum_recv.at[z, lower], j * inner + p, core * n)

        def shared():
            for load in loads[5:8]:
                load.wait()
            inputs = normed[...]
            hidden = silu_product(dot(inputs, sgate_w[...]), dot(inputs, sup_w[...]))
            shared_out[:, given] = dot(hidden, sdown_w[:, given]).astype(BF16)
            here = shared_out.at[:, given]
            send(here, shared_in.at[:, given], 5, core_sem.at[0], ep, other)
            shared_out[:, kept] = dot(hidden, sdown_w[:, kept]).astype(BF16)

        def step(task, *what):
            with jax.named_scope(task.__name__ + "".join(str(w) for w in what)):
                task(*what)

        for task, *what in PLAN(core, outer, dispatch, shared, pair, begin, finish, settle, give_back, combine):
            step(task, *what)

        with jax.named_scope("own"):
            weights = weighed[0]
            mixed_rows = [gathered(0, weights, n, piece) for n, piece in enumerate(my_pieces)]
            lent = pl.ds(split, half - split)
            if core == 1:
                sum_out[outer - 1, :, lent] = mixed_rows[0].astype(BF16)
                here = sum_out.at[outer - 1, :, lent]
                send(here, sum_in.at[z, :, lent], 7, sum_recv.at[z, 1], ep, 0)
            owned = [(my_pieces[core], 0)]
            arrive(shared_in.at[:, kept], core_sem.at[0])
            shared_rows = shared_out[:, kept].astype(F32) + shared_in[:, kept].astype(F32)
            shared_rows = shared_rows.astype(BF16).astype(F32)
            totals = [mixed_rows[core] + shared_rows[:, : my_pieces[core].size]]
            if core == 0:
                arrive(sum_in.at[z, :, lent], sum_recv.at[z, 1])
                totals.append(shared_rows[:, split:] + sum_in[z, :, lent].astype(F32))
                owned.append((lent, 1))
        with jax.named_scope("sums"):
            for i in range(1, outer):
                j = passing[i]
                for k, (piece, n) in enumerate(owned):
                    arrive(sum_in.at[j, :, piece], sum_recv.at[j, n])
                    totals[k] = totals[k] + sum_in[j, :, piece].astype(F32)
        combined = totals[0] if len(totals) == 1 else jnp.concatenate(totals, axis=1)

        own_squares = jnp.sum(combined * combined, axis=1, keepdims=True)
        last_out[...] = jnp.broadcast_to(own_squares, last_out.shape)
        send(last_out, last_in, 6, core_sem.at[1], ep, other)
        scaled = combined * out_gain[...].astype(F32)[None, :]
        with jax.named_scope("lastwait"):
            arrive(last_in, core_sem.at[1])
        squares = own_squares + last_in[:, :1]
        mixed[...] = (scaled * lax.rsqrt(squares / width + EPSILON)).astype(BF16)

        for copies in sorted(set(column_sends(outer))):
            planes = [plane for plane, n in enumerate(column_sends(outer)) if n == copies]

            @pl.when(functools.reduce(jnp.logical_or, [z == plane for plane in planes]))
            def _(copies=copies):
                sent(column.at[pl.ds(0, copies), :, sent_at], 8)

        sent(staged.at[:, pl.ds(0, inner - 1), :, mine], 0)
        sent(rows_in.at[:, :, :, mine], 1)
        sent(part_out.at[:, :, :, theirs], 2)
        sent(result.at[:, pl.ds(0, inner - 1), :, mine], 3)
        sent(sum_out.at[pl.ds(0, outer - 1), :, mine], 4)
        sent(shared_out.at[:, given], 5)
        sent(last_out, 6)
        if core == 1:
            sent(sum_out.at[outer - 1, :, lent], 7)

    for core in range(2):

        @pl.when(tp == core)
        def _(core=core):
            on_core(core)


def plan(core, outer, dispatch, shared, pair, begin, finish, settle, give_back, combine):
    steps = [(dispatch, 0), (shared,), (dispatch, 1)]
    for i in range(2, outer):
        steps += [(dispatch, i, True)] if i == outer - 1 else []
        steps += [(pair, i - 2), (dispatch, i, False)]
    steps += [(pair, i) for i in range(max(0, outer - 2), 2)]
    steps += [(begin, 0, 1), (finish, 0, 1), (settle, 0, 1)]
    steps += [(pair, 2)] if 2 >= outer - 2 and outer > 2 else []
    for i in range(2, outer):
        earlier = [(give_back, 1), (give_back, 0)] if i == 2 else [(give_back, i - 1)]
        steps += [(begin, i)]
        steps += [(finish, i)] + earlier if core and i > 2 else earlier + [(finish, i)]
        steps += [(settle, i)]
    steps += [(give_back, outer - 1)]
    steps += [(combine, i) for i in range(1, outer)]
    return steps


PLAN = plan
SPLIT = 2
DELAY = (0, 600)


def body(
    experts,
    tokens,
    in_gain,
    route_expert,
    route_weight,
    gate_weight,
    up_weight,
    down_weight,
    shared_gate,
    shared_up,
    shared_down,
    out_gain,
):
    inner = 1
    while inner * inner < experts:
        inner *= 2
    outer = experts // inner
    local_tokens, width = tokens.shape
    half = width // 2
    split = width * SPLIT // 16
    top_count = route_expert.shape[1]
    capacity = max(2, (local_tokens * top_count * 4 + 3 * experts - 1) // (3 * experts))
    cap = -(-capacity // 16) * 16
    info_width = -(-3 * experts // 128) * 128
    hidden = gate_weight.shape[2]
    shared_width = shared_gate.shape[1]

    def vm(shape, kind=BF16):
        return pltpu.VMEM(shape, kind)

    grid_rows = (outer, inner, cap, width)
    most = 2
    dma = pltpu.SemaphoreType.DMA
    in_vmem = pl.BlockSpec(memory_space=pltpu.VMEM)
    in_hbm = pl.BlockSpec(memory_space=pltpu.HBM)
    return pl.pallas_call(
        functools.partial(kernel, outer, inner, cap, info_width, split),
        out_shape=pltpu.VMEM((local_tokens, half), BF16),
        in_specs=[in_hbm] * 11,
        out_specs=in_vmem,
        scratch_shapes=[
            vm((local_tokens, width)),
            vm((width,)),
            vm((top_count, local_tokens), jnp.int32),
            vm((top_count, local_tokens), F32),
            vm((half,)),
            vm((width, hidden)),
            vm((width, hidden)),
            vm((hidden, width)),
            vm((width, shared_width)),
            vm((width, shared_width)),
            vm((shared_width, width)),
            vm((local_tokens, width)),
            vm((outer, local_tokens, width + info_width)),
            vm(grid_rows),
            vm(grid_rows),
            vm(grid_rows),
            vm(grid_rows),
            vm(grid_rows),
            vm(grid_rows),
            vm(grid_rows),
            vm((outer, local_tokens, width)),
            vm((outer, local_tokens, width)),
            vm((local_tokens, width)),
            vm((local_tokens, width)),
            vm((local_tokens, 128), F32),
            vm((local_tokens, 128), F32),
            dma((11,)),
            dma((outer,)),
            dma((outer,)),
            dma((outer,)),
            dma((outer, most)),
            dma((outer, most)),
            dma((outer, most)),
            dma((9,)),
            dma((2,)),
        ],
        compiler_params=pltpu.CompilerParams(
            collective_id=0, has_side_effects=True, vmem_limit_bytes=60 * 1024 * 1024
        ),
    )(
        tokens,
        in_gain,
        route_expert.T,
        route_weight.T,
        out_gain,
        gate_weight,
        up_weight,
        down_weight,
        shared_gate,
        shared_up,
        shared_down,
    )


def solution(mesh):
    return jax.shard_map(
        functools.partial(body, mesh.shape["ep"]),
        mesh=mesh,
        in_specs=(
            P(("grp", "ep"), None),
            P(),
            P(("grp", "ep"), None),
            P(("grp", "ep"), None),
            P("ep", None, "tp"),
            P("ep", None, "tp"),
            P("ep", "tp", None),
            P(None, "tp"),
            P(None, "tp"),
            P("tp", None),
            P("tp"),
        ),
        out_specs=P(("grp", "ep"), "tp"),
        check_vma=False,
    )
```

```python
import functools

import jax
import jax.numpy as jnp
from jax import lax
from jax.experimental import pallas as pl
from jax.experimental.pallas import tpu as pltpu
from jax.sharding import PartitionSpec as P

EPSILON = 1e-06
F32 = jnp.float32
BF16 = jnp.bfloat16


def dot(a, b):
    return jnp.dot(a, b, preferred_element_type=F32)


def dot_t(a, b):
    return lax.dot_general(a, b, (((1,), (1,)), ((), ())), preferred_element_type=F32)


def silu_product(gate_value, upward):
    return (gate_value * (1.0 / (1.0 + jnp.exp(-gate_value))) * upward).astype(BF16)


def column_sends(outer):
    counts = []
    for z in range(outer):
        straight = [j for j in range(outer) if j != z and (z == 0 or abs(j - z) != 2)]
        passed = [j for j in (z - 1, z + 1) if 0 < j < outer and 0 <= 2 * z - j < outer]
        counts.append(len(straight) + len(passed))
    return counts


def kernel(
    outer,
    inner,
    cap,
    info_width,
    split,
    tokens_hbm,
    in_gain_hbm,
    route_expert_hbm,
    route_weight_hbm,
    out_gain_hbm,
    gate_hbm,
    up_hbm,
    down_hbm,
    sgate_hbm,
    sup_hbm,
    sdown_hbm,
    mixed,
    tokens,
    in_gain,
    route_expert,
    route_weight,
    out_gain,
    gate_w,
    up_w,
    down_w,
    sgate_w,
    sup_w,
    sdown_w,
    normed,
    column,
    staged,
    rows_in,
    part_out,
    part_in,
    part_own,
    result,
    back,
    sum_out,
    sum_in,
    shared_out,
    shared_in,
    last_out,
    last_in,
    w_sem,
    col_recv,
    plane_recv,
    pair_recv,
    part_recv,
    back_recv,
    sum_recv,
    send_sem,
    core_sem,
):
    ep = lax.axis_index("ep")
    tp = lax.axis_index("tp")
    z = ep // inner
    p = ep % inner
    experts = outer * inner
    local_tokens, width = tokens.shape
    half = width // 2

    loads = [
        pltpu.make_async_copy(src, dst, w_sem.at[i])
        for i, (src, dst) in enumerate(
            [
                (tokens_hbm, tokens),
                (in_gain_hbm, in_gain),
                (route_expert_hbm, route_expert),
                (route_weight_hbm, route_weight),
                (out_gain_hbm, out_gain),
                (sgate_hbm, sgate_w),
                (sup_hbm, sup_w),
                (sdown_hbm, sdown_w),
                (gate_hbm.at[0], gate_w),
                (up_hbm.at[0], up_w),
                (down_hbm.at[0], down_w),
            ]
        )
    ]
    for load in loads[:5]:
        load.start()

    barrier = pltpu.get_barrier_semaphore()

    def greet(ep_to, tp_to):
        pl.semaphore_signal(
            barrier, inc=1, device_id={"ep": ep_to, "tp": tp_to}, device_id_type=pl.DeviceIdType.MESH
        )

    for d in range(1, outer):
        greet(lax.rem(z + d, outer) * inner + p, tp)
    for d in range(1, inner):
        greet(z * inner + lax.rem(p + d, inner), tp)
    greet(ep, 1 - tp)

    for load in loads[:5]:
        load.wait()
    for load in loads[5:]:
        load.start()
    floats = tokens[...].astype(F32)
    mean = jnp.sum(floats * floats, axis=1, keepdims=True) / width
    rows = (floats * lax.rsqrt(mean + EPSILON) * in_gain[...].astype(F32)[None, :]).astype(BF16)
    normed[...] = rows

    fact = lax.broadcasted_iota(jnp.int32, (info_width, local_tokens), 0)
    fact_expert = lax.rem(fact, experts)
    named = jnp.zeros((info_width, local_tokens), F32)
    weight = jnp.zeros((info_width, local_tokens), F32)
    for k in range(route_expert.shape[0]):
        hit = route_expert[k : k + 1, :] == fact_expert
        named = named + jnp.where(hit, 1.0, 0.0)
        weight = weight + jnp.where(hit, route_weight[k : k + 1, :], 0.0)
    row_i = lax.broadcasted_iota(jnp.int32, (local_tokens, local_tokens), 0)
    col_i = lax.broadcasted_iota(jnp.int32, (local_tokens, local_tokens), 1)
    upto = jnp.where(row_i <= col_i, 1.0, 0.0).astype(BF16)
    place = dot(named.astype(BF16), upto) * named
    high = weight.astype(BF16).astype(F32)
    facts = jnp.where(fact < experts, place, jnp.where(fact < 2 * experts, high, weight - high))
    facts = jnp.where(fact < 3 * experts, facts, 0.0).astype(BF16)
    same = jnp.where(row_i == col_i, 1.0, 0.0).astype(BF16)
    info = dot_t(same, facts).astype(BF16)

    short = jnp.minimum(z, outer - 1 - z)

    def nth(i):
        if i == 0:
            return z
        near = -((i + 1) // 2) if i % 2 else i // 2
        far = jnp.where(z < outer - 1 - z, i - short, short - i)
        if i > 1:
            ends = i + 1 if i < outer - 1 else 2
            far = jnp.where(short > 0, far, jnp.where(z == 0, ends, -ends))
        return z + jnp.where(i <= 2 * short, near, far)

    order = [nth(i) for i in range(outer)]
    passing = list(order)
    if outer > 3:
        swap = z == outer - 2
        passing[-2:] = [jnp.where(swap, order[-1], order[-2]), jnp.where(swap, order[-2], order[-1])]

    def direct(to):
        return (z == 0) | ((to - z) * (to - z) != 4)

    def passes(j):
        on = 2 * z - j
        return on, ((j - z) * (j - z) == 1) & (on >= 0) & (on < outer) & (j > 0)

    slots = inner * cap
    slot_row = lax.broadcasted_iota(jnp.int32, (slots, info_width), 0)
    slot_lane = lax.broadcasted_iota(jnp.int32, (slots, info_width), 1)
    slot_expert = z * inner + slot_row // cap

    def selector(offset):
        return jnp.where(slot_lane == slot_expert + offset, 1.0, 0.0).astype(BF16)

    slot_rank = (lax.broadcasted_iota(jnp.int32, (slots, local_tokens), 0) % cap + 1).astype(F32)
    slot_of_lane = (lax.broadcasted_iota(jnp.int32, (local_tokens, slots), 1) % cap + 1).astype(F32)

    peers = [e + jnp.where(e < p, 0, 1) for e in range(inner - 1)]


    def on_core(core):
        edges = (0, split, width)
        first, end = edges[core], edges[core + 1]
        count = end - first
        other = 1 - core
        mine = pl.ds(first, count)
        theirs = pl.ds(edges[other], edges[other + 1] - edges[other])
        kept = pl.ds(core * half, half)
        given = pl.ds(other * half, half)
        facts_at = pl.ds(first, info_width)
        rows_at = pl.ds(first + info_width, count)
        sent_at = pl.ds(first, info_width + count)

        def pieces(which):
            if which == 0:
                return [pl.ds(0, split)]
            return [pl.ds(split, half - split), pl.ds(half, half)]

        my_pieces = pieces(core)
        pl.semaphore_wait(barrier, outer + inner - 1)

        column[z, :, facts_at] = info
        column[z, :, rows_at] = rows[:, first:end]

        def remote(src, dst, send, recv, ep_to, tp_to):
            return pltpu.make_async_remote_copy(
                src_ref=src,
                dst_ref=dst,
                send_sem=send,
                recv_sem=recv,
                device_id={"ep": ep_to, "tp": tp_to},
                device_id_type=pl.DeviceIdType.MESH,
            )

        def send(src, dst, kind, recv_sem, ep_to, tp_to):
            remote(src, dst, send_sem.at[kind], recv_sem, ep_to, tp_to).start()

        def arrive(ref, recv_sem):
            with jax.named_scope("w"):
                remote(ref, ref, send_sem.at[0], recv_sem, ep, other).wait_recv()

        def sent(ref, kind):
            remote(ref, ref, send_sem.at[kind], col_recv.at[0], ep, other).wait_send()

        def column_copy(block, to):
            here = column.at[block, :, sent_at]
            return remote(here, here, send_sem.at[8], col_recv.at[block], to * inner + p, core)

        for i, to in enumerate(order[1:], 1):
            to = jnp.where(z == 0, i, to)

            @pl.when(direct(to))
            def _(to=to):
                column_copy(z, to).start()

        pick_place = selector(0)
        pick_high = selector(experts)
        pick_low = selector(2 * experts)

        def dispatch(i, early=None):
            if i < outer - 1 or i == 1:
                move(i)
            else:

                @pl.when((z == outer - 2) == early)
                def _():
                    move(i)

        def move(i):
            j = order[i]
            if i:
                arrive(column.at[j, :, sent_at], col_recv.at[j])
                on, wanted = passes(j)

                @pl.when(wanted)
                def _():
                    column_copy(j, on).start()

            where = dot_t(pick_place, column[j, :, facts_at])
            onehot = jnp.where(where == slot_rank, 1.0, 0.0).astype(BF16)
            moved = dot(onehot, column[j, :, rows_at]).astype(BF16)
            staged[j, :, :, mine] = moved.reshape(inner, cap, count)
            for to in peers:
                send(
                    staged.at[j, to, :, mine],
                    rows_in.at[j, p, :, mine],
                    0,
                    plane_recv.at[j],
                    z * inner + to,
                    core,
                )
            rows_in[j, p, :, mine] = staged[j, p, :, mine]

        def pair(i):
            j = passing[i]
            arrive(rows_in.at[j, pl.ds(0, inner - 1), :, mine], plane_recv.at[j])
            here = rows_in.at[j, :, :, mine]
            send(here, here, 1, pair_recv.at[j], ep, other)

        opened = {}

        def begin(*group):
            if group[0] == 0:
                for load in loads[8:]:
                    load.wait()

            def rows_of(columns):
                blocks = [rows_in[passing[i], :, :, columns].reshape(slots, columns.size) for i in group]
                return blocks[0] if len(blocks) == 1 else jnp.concatenate(blocks, axis=0)

            own_rows = rows_of(mine)
            gate_value = dot(own_rows, gate_w[mine, :])
            upward = dot(own_rows, up_w[mine, :])
            opened[group] = gate_value, upward, rows_of

        def finish(*group):
            gate_value, upward, rows_of = opened[group]
            for i in group:
                j = passing[i]
                arrive(rows_in.at[j, :, :, theirs], pair_recv.at[j])
            other_rows = rows_of(theirs)
            gate_value = gate_value + dot(other_rows, gate_w[theirs, :])
            upward = upward + dot(other_rows, up_w[theirs, :])
            if len(group) == 1 and outer - 2 <= group[0] + 1 < outer:
                pair(group[0] + 1)
            opened[group] = silu_product(gate_value, upward)
            for n, piece in enumerate(pieces(other)):
                store(group, part_out, piece)
                for i in reversed(group):
                    j = passing[i]
                    here = part_out.at[j, :, :, piece]
                    send(here, part_in.at[j, :, :, piece], 2, part_recv.at[j, n], ep, other)

        def settle(*group):
            for piece in my_pieces:
                store(group, part_own, piece)

        def store(group, target, columns):
            values = dot(opened[group], down_w[:, columns]).astype(BF16)
            for n, i in enumerate(group):
                block = values[n * slots : (n + 1) * slots]
                target[passing[i], :, :, columns] = block.reshape(inner, cap, columns.size)

        def give_back(i):
            j = passing[i]
            if i == outer - 1:
                for k in [0] + list(range(2, outer)):
                    weighed[k] = weigh(k)
            if i == 1:
                weighed[1] = weigh(1)
            for n, piece in enumerate(my_pieces):
                arrive(part_in.at[j, :, :, piece], part_recv.at[j, n])
                total = part_own[j, :, :, piece].astype(F32) + part_in[j, :, :, piece].astype(F32)
                result[j, :, :, piece] = total.astype(BF16)
                for to in peers:
                    send(
                        result.at[j, to, :, piece],
                        back.at[j, p, :, piece],
                        3,
                        back_recv.at[j, n],
                        z * inner + to,
                        core,
                    )
                back[j, p, :, piece] = result[j, p, :, piece]

        weighed = {}

        def weigh(i):
            known = column[passing[i], :, facts_at]
            chosen = dot_t(known, pick_place) == slot_of_lane
            high_part = jnp.where(chosen, dot_t(known, pick_high), 0.0).astype(BF16)
            low_part = jnp.where(chosen, dot_t(known, pick_low), 0.0).astype(BF16)
            return jnp.concatenate([high_part, low_part], axis=0)

        def gathered(i, weights, n, piece):
            j = passing[i]
            arrive(back.at[j, pl.ds(0, inner - 1), :, piece], back_recv.at[j, n])
            values = back[j, :, :, piece].reshape(slots, piece.size)
            both = dot(weights, values)
            return both[:local_tokens] + both[local_tokens:]

        def combine(i):
            j = passing[i]
            weights = weighed.pop(i)
            for n, piece in enumerate(my_pieces):
                sum_out[i - 1, :, piece] = gathered(i, weights, n, piece).astype(BF16)
                if i == outer - 1 and n == 0:

                    for end, cycles in ((0, DELAY[0]), (outer - 1, DELAY[1])):

                        @pl.when(z == end)
                        def _(cycles=cycles):
                            pl.delay(cycles)

                here = sum_out.at[i - 1, :, piece]
                lower = core - core * n
                send(here, sum_in.at[z, :, piece], 4, sum_recv.at[z, lower], j * inner + p, core * n)

        def shared():
            for load in loads[5:8]:
                load.wait()
            inputs = normed[...]
            hidden = silu_product(dot(inputs, sgate_w[...]), dot(inputs, sup_w[...]))
            shared_out[:, given] = dot(hidden, sdown_w[:, given]).astype(BF16)
            here = shared_out.at[:, given]
            send(here, shared_in.at[:, given], 5, core_sem.at[0], ep, other)
            shared_out[:, kept] = dot(hidden, sdown_w[:, kept]).astype(BF16)

        def step(task, *what):
            with jax.named_scope(task.__name__ + "".join(str(w) for w in what)):
                task(*what)

        for task, *what in PLAN(core, outer, dispatch, shared, pair, begin, finish, settle, give_back, combine):
            step(task, *what)

        with jax.named_scope("own"):
            weights = weighed[0]
            mixed_rows = [gathered(0, weights, n, piece) for n, piece in enumerate(my_pieces)]
            lent = pl.ds(split, half - split)
            if core == 1:
                sum_out[outer - 1, :, lent] = mixed_rows[0].astype(BF16)
                here = sum_out.at[outer - 1, :, lent]
                send(here, sum_in.at[z, :, lent], 7, sum_recv.at[z, 1], ep, 0)
            owned = [(my_pieces[core], 0)]
            arrive(shared_in.at[:, kept], core_sem.at[0])
            shared_rows = shared_out[:, kept].astype(F32) + shared_in[:, kept].astype(F32)
            shared_rows = shared_rows.astype(BF16).astype(F32)
            totals = [mixed_rows[core] + shared_rows[:, : my_pieces[core].size]]
            if core == 0:
                arrive(sum_in.at[z, :, lent], sum_recv.at[z, 1])
                totals.append(shared_rows[:, split:] + sum_in[z, :, lent].astype(F32))
                owned.append((lent, 1))
        with jax.named_scope("sums"):
            for i in range(1, outer):
                j = passing[i]
                for k, (piece, n) in enumerate(owned):
                    arrive(sum_in.at[j, :, piece], sum_recv.at[j, n])
                    totals[k] = totals[k] + sum_in[j, :, piece].astype(F32)
        combined = totals[0] if len(totals) == 1 else jnp.concatenate(totals, axis=1)

        own_squares = jnp.sum(combined * combined, axis=1, keepdims=True)
        last_out[...] = jnp.broadcast_to(own_squares, last_out.shape)
        send(last_out, last_in, 6, core_sem.at[1], ep, other)
        scaled = combined * out_gain[...].astype(F32)[None, :]
        with jax.named_scope("lastwait"):
            arrive(last_in, core_sem.at[1])
        squares = own_squares + last_in[:, :1]
        mixed[...] = (scaled * lax.rsqrt(squares / width + EPSILON)).astype(BF16)

        for copies in sorted(set(column_sends(outer))):
            planes = [plane for plane, n in enumerate(column_sends(outer)) if n == copies]

            @pl.when(functools.reduce(jnp.logical_or, [z == plane for plane in planes]))
            def _(copies=copies):
                sent(column.at[pl.ds(0, copies), :, sent_at], 8)

        sent(staged.at[:, pl.ds(0, inner - 1), :, mine], 0)
        sent(rows_in.at[:, :, :, mine], 1)
        sent(part_out.at[:, :, :, theirs], 2)
        sent(result.at[:, pl.ds(0, inner - 1), :, mine], 3)
        sent(sum_out.at[pl.ds(0, outer - 1), :, mine], 4)
        sent(shared_out.at[:, given], 5)
        sent(last_out, 6)
        if core == 1:
            sent(sum_out.at[outer - 1, :, lent], 7)

    for core in range(2):

        @pl.when(tp == core)
        def _(core=core):
            on_core(core)


def plan(core, outer, dispatch, shared, pair, begin, finish, settle, give_back, combine):
    steps = [(dispatch, 0), (shared,), (dispatch, 1)]
    for i in range(2, outer):
        steps += [(dispatch, i, True)] if i == outer - 1 else []
        steps += [(pair, i - 2), (dispatch, i, False)]
    steps += [(pair, i) for i in range(max(0, outer - 2), 2)]
    steps += [(begin, 0, 1), (finish, 0, 1), (settle, 0, 1)]
    steps += [(pair, 2)] if 2 >= outer - 2 and outer > 2 else []
    for i in range(2, outer):
        earlier = [(give_back, 1), (give_back, 0)] if i == 2 else [(give_back, i - 1)]
        steps += [(begin, i)]
        steps += [(finish, i)] + earlier if core and i > 2 else earlier + [(finish, i)]
        steps += [(settle, i)]
    steps += [(give_back, outer - 1)]
    steps += [(combine, i) for i in range(1, outer)]
    return steps


PLAN = plan
SPLIT = 2
DELAY = (0, 300)


def body(
    experts,
    tokens,
    in_gain,
    route_expert,
    route_weight,
    gate_weight,
    up_weight,
    down_weight,
    shared_gate,
    shared_up,
    shared_down,
    out_gain,
):
    inner = 1
    while inner * inner < experts:
        inner *= 2
    outer = experts // inner
    local_tokens, width = tokens.shape
    half = width // 2
    split = width * SPLIT // 16
    top_count = route_expert.shape[1]
    capacity = max(2, (local_tokens * top_count * 4 + 3 * experts - 1) // (3 * experts))
    cap = -(-capacity // 16) * 16
    info_width = -(-3 * experts // 128) * 128
    hidden = gate_weight.shape[2]
    shared_width = shared_gate.shape[1]

    def vm(shape, kind=BF16):
        return pltpu.VMEM(shape, kind)

    grid_rows = (outer, inner, cap, width)
    most = 2
    dma = pltpu.SemaphoreType.DMA
    in_vmem = pl.BlockSpec(memory_space=pltpu.VMEM)
    in_hbm = pl.BlockSpec(memory_space=pltpu.HBM)
    return pl.pallas_call(
        functools.partial(kernel, outer, inner, cap, info_width, split),
        out_shape=pltpu.VMEM((local_tokens, half), BF16),
        in_specs=[in_hbm] * 11,
        out_specs=in_vmem,
        scratch_shapes=[
            vm((local_tokens, width)),
            vm((width,)),
            vm((top_count, local_tokens), jnp.int32),
            vm((top_count, local_tokens), F32),
            vm((half,)),
            vm((width, hidden)),
            vm((width, hidden)),
            vm((hidden, width)),
            vm((width, shared_width)),
            vm((width, shared_width)),
            vm((shared_width, width)),
            vm((local_tokens, width)),
            vm((outer, local_tokens, width + info_width)),
            vm(grid_rows),
            vm(grid_rows),
            vm(grid_rows),
            vm(grid_rows),
            vm(grid_rows),
            vm(grid_rows),
            vm(grid_rows),
            vm((outer, local_tokens, width)),
            vm((outer, local_tokens, width)),
            vm((local_tokens, width)),
            vm((local_tokens, width)),
            vm((local_tokens, 128), F32),
            vm((local_tokens, 128), F32),
            dma((11,)),
            dma((outer,)),
            dma((outer,)),
            dma((outer,)),
            dma((outer, most)),
            dma((outer, most)),
            dma((outer, most)),
            dma((9,)),
            dma((2,)),
        ],
        compiler_params=pltpu.CompilerParams(
            collective_id=0, has_side_effects=True, vmem_limit_bytes=60 * 1024 * 1024,
        ),
    )(
        tokens,
        in_gain,
        route_expert.T,
        route_weight.T,
        out_gain,
        gate_weight,
        up_weight,
        down_weight,
        shared_gate,
        shared_up,
        shared_down,
    )


def solution(mesh):
    return jax.shard_map(
        functools.partial(body, mesh.shape["ep"]),
        mesh=mesh,
        in_specs=(
            P(("grp", "ep"), None),
            P(),
            P(("grp", "ep"), None),
            P(("grp", "ep"), None),
            P("ep", None, "tp"),
            P("ep", None, "tp"),
            P("ep", "tp", None),
            P(None, "tp"),
            P(None, "tp"),
            P("tp", None),
            P("tp"),
        ),
        out_specs=P(("grp", "ep"), "tp"),
        check_vma=False,
    )
```
